32 devices in a mesh: grp: 2 (over x), tp: 16 (over z, y, core).
Axes of the slice: x: 2, y: 2, z: 4, core: 2. Of those that a mesh axis runs over, the one named last changes fastest.
Arguments:
- tokens: bfloat16 [3072, 2048], P('grp', 'tp'), parts along dimension 0, may hold values from -6 to 6
- lengths: int32 [192], P('grp'), parts along dimension 0, may hold values from 1 to 16, 960 in all
- gain_first: float32 [2048], replicated, may hold values from 0.1 to 1.9
- query_first: bfloat16 [2048, 1024], P(None, 'tp'), may hold values from -0.125 to 0.125
- key_first: bfloat16 [2048, 1024], P(None, 'tp'), may hold values from -0.125 to 0.125
- value_first: bfloat16 [2048, 2048], P(None, 'tp'), may hold values from -0.125 to 0.125
- gate_first: bfloat16 [2048, 2048], P(None, 'tp'), may hold values from -0.125 to 0.125
- out_first: bfloat16 [2048, 2048], P('tp'), may hold values from -0.1875 to 0.1875
- state_first: float32 [192, 16, 64, 128], P('grp', 'tp'), parts along dimension 0, may hold values from -0.9 to 0.9
- gain_second: float32 [2048], replicated, may hold values from 0.1 to 1.9
- query_second: bfloat16 [2048, 1024], P(None, 'tp'), may hold values from -0.125 to 0.125
- key_second: bfloat16 [2048, 1024], P(None, 'tp'), may hold values from -0.125 to 0.125
- value_second: bfloat16 [2048, 2048], P(None, 'tp'), may hold values from -0.125 to 0.125
- gate_second: bfloat16 [2048, 2048], P(None, 'tp'), may hold values from -0.125 to 0.125
- out_second: bfloat16 [2048, 2048], P('tp'), may hold values from -0.1875 to 0.1875
- state_second: float32 [192, 16, 64, 128], P('grp', 'tp'), parts along dimension 0, may hold values from -0.9 to 0.9
Outputs:
- mixed_out: bfloat16 [3072, 2048], P('grp', 'tp'), parts along dimension 0
- state_first_new: float32 [192, 16, 64, 128], P('grp', 'tp'), parts along dimension 0
- state_second_new: float32 [192, 16, 64, 128], P('grp', 'tp'), parts along dimension 0
The draws below stay inside these ranges and needn't reach their ends.
There are 2 independent parts, one for each index of `grp`. The reference program is written for one: setup_inputs(seed, part) draws one part's arguments, and reference() takes and returns one part's arrays. A program takes and returns all parts, laid end to end along the dimension named above; an argument that names none is the same for every part. Nothing has to cross between parts.
All inputs are finite; a program needn't handle non-finite values.
Results may differ from the reference program's by a relative error of at most 0.025.
Values may be sent and summed in bfloat16 or wider, within the bound.
A program may use at most 128 MiB of HBM per device.

```python
import math
import jax
import jax.numpy as jnp
import numpy as np
from jax import lax

D = 2048
DK = 64
DV = 128
HEADS = 16
BATCH = 96
BLOCK = 16
PAST_LEN = 16384
ROWS = 1536
LIVE_TOTAL = 960


def raised(values, key, source, target, shards_of, factor):
    owner, partner = [(jnp.arange(values.shape[axis_at]) // (values.shape[axis_at] // shards_of)).reshape([-1 if axis == axis_at else 1 for axis in range(values.ndim)]) for axis_at in (source, target)]
    chosen = jax.random.permutation(key, shards_of)[partner]
    strong = (owner == chosen) | (owner == (partner + shards_of // 2) % shards_of)
    return jnp.where(strong, factor * values, values)


def steps_of(stream_key, dims, shards, least, largest):
    def one(position, blocks):
        steps = jax.random.uniform(jax.random.fold_in(jax.random.fold_in(stream_key, 6), position), (blocks,), jnp.float32, least / len(shards), largest / len(shards))
        return jnp.repeat(jnp.exp(steps), dims[position] // blocks).reshape((-1,) + (1,) * (len(dims) - position - 1))

    factor_of = one(*shards[0])
    for cut in shards[1:]:
        factor_of = factor_of * one(*cut)
    return factor_of


def profile(number_of, total, bound, lean):
    loads = [(1 << 20) // math.isqrt(rank ** lean) + 1 for rank in range(2, number_of + 1)]
    rest, given = total - bound - (number_of - 1), [1] * (number_of - 1)
    while rest > 0:
        candidates = [i for i in range(number_of - 1) if given[i] < bound]
        whole, remaining = sum([loads[i] for i in candidates]), rest
        for i in candidates:
            extra = min(bound - given[i], max(1, remaining * loads[i] // whole), rest)
            given[i] = given[i] + extra
            rest = rest - extra
    return np.array([bound] + given)


def ragged_sizes(key, number_of, total, most, slope):
    if number_of == 2:
        one = jax.random.randint(key, (), max(1, total - most), min(most, total - 1) + 1)
        return jnp.stack([one, total - one])
    sizes = jnp.asarray(profile(number_of, total, most, slope), jnp.int32)
    couples = (number_of - 1) // 2
    giver, taker = sizes[1:1 + 2 * couples:2], sizes[2:2 + 2 * couples:2]
    margin = jnp.minimum(giver - 1, most - taker)
    shifted = jax.random.randint(jax.random.fold_in(key, 1), (couples,), 0, 1 << 20) % (margin + 1)
    sizes = sizes.at[1:1 + 2 * couples:2].set(giver - shifted).at[2:2 + 2 * couples:2].set(taker + shifted)
    return sizes[jax.random.permutation(jax.random.fold_in(key, 2), number_of)]


def centred(key, dims, spread, reach, cuts=(), held_as=jnp.bfloat16):
    values = jax.random.normal(key, dims, jnp.float32) * spread
    if len(cuts) > 0:
        values = steps_of(key, dims, cuts, -0.22, 0.18) * values
    return jnp.clip(values, min=-reach, max=reach).astype(held_as)


def heavy_noise(rng, dims, scale, most, pieces, heavy, kind=jnp.bfloat16):
    entries = scale * jax.random.normal(rng, dims, jnp.float32)
    if pieces:
        entries = entries * steps_of(rng, dims, pieces, -0.22, 0.18)
    return jnp.clip(raised(entries, jax.random.fold_in(rng, 3), *heavy), -most, most).astype(kind)


def setup_inputs(seed: int = 0, part: int = 0) -> dict:
    key_of = jax.random.split(jax.random.key(seed), 17)
    own_keys = jax.random.split(jax.random.fold_in(key_of[16], part), 17)
    return {
        "tokens": centred(own_keys[0], (ROWS, D), 1.0, 6.0, ((1, 16),)),
        "lengths": ragged_sizes(own_keys[1], BATCH, LIVE_TOTAL, BLOCK, 2).astype(jnp.int32),
        "gain_first": jnp.clip(1.0 + 0.18 * jax.random.normal(key_of[2], (D,), jnp.float32), 0.1, 1.9),
        "query_first": centred(key_of[3], (D, HEADS * DK), D ** -0.5, 0.125, ((1, 16),)),
        "key_first": centred(key_of[4], (D, HEADS * DK), D ** -0.5, 0.125, ((1, 16),)),
        "value_first": centred(key_of[5], (D, HEADS * DV), D ** -0.5, 0.125, ((1, 16),)),
        "gate_first": centred(key_of[6], (D, HEADS * DV), D ** -0.5, 0.125, ((1, 16),)),
        "out_first": heavy_noise(key_of[7], (HEADS * DV, D), (HEADS * DV) ** -0.5, 0.1875, ((0, 16),), (0, 1, 16, 2.0)),
        "state_first": centred(own_keys[8], (BATCH, HEADS, DK, DV), 0.15, 0.9, ((1, 16),), jnp.float32),
        "gain_second": jnp.clip(1.0 + 0.18 * jax.random.normal(key_of[9], (D,), jnp.float32), 0.1, 1.9),
        "query_second": centred(key_of[10], (D, HEADS * DK), D ** -0.5, 0.125, ((1, 16),)),
        "key_second": centred(key_of[11], (D, HEADS * DK), D ** -0.5, 0.125, ((1, 16),)),
        "value_second": centred(key_of[12], (D, HEADS * DV), D ** -0.5, 0.125, ((1, 16),)),
        "gate_second": centred(key_of[13], (D, HEADS * DV), D ** -0.5, 0.125, ((1, 16),)),
        "out_second": heavy_noise(key_of[14], (HEADS * DV, D), (HEADS * DV) ** -0.5, 0.1875, ((0, 16),), (0, 1, 16, 2.0)),
        "state_second": centred(own_keys[15], (BATCH, HEADS, DK, DV), 0.15, 0.9, ((1, 16),), jnp.float32),
    }


NORM_EPSILON = 1e-06
ROPE_BASE = 10000.0

def norm_rows(rows_in, gain_vec):
    rows_f = rows_in.astype(jnp.float32)
    inv_rms = lax.rsqrt(lax.optimization_barrier(jnp.mean(rows_f * rows_f, axis=-1, keepdims=True)) + NORM_EPSILON)
    return (rows_f * inv_rms * gain_vec.astype(jnp.float32)).astype(jnp.bfloat16)

def rotate(vectors):
    half_dim = vectors.shape[-1] // 2
    inverse = ROPE_BASE ** (-jnp.arange(half_dim, dtype=jnp.float32) / half_dim)
    positions = PAST_LEN + jnp.arange(vectors.shape[1], dtype=jnp.float32)
    angles = positions[:, None] * inverse[None, :]
    cosine_table = jnp.cos(angles)[None, :, None, :]
    sine_table = jnp.sin(angles)[None, :, None, :]
    front_half = vectors[..., :half_dim]
    back_half = vectors[..., half_dim:]
    return jnp.concatenate([front_half * cosine_table - back_half * sine_table, front_half * sine_table + back_half * cosine_table], axis=-1)

def decay_logs(head_total):
    head_ids = jnp.arange(head_total).astype(jnp.float32)
    return jnp.log(1.0 - 2.0 ** (-1.5 - 6.0 * head_ids / (head_total - 1)))

def retain(normed, lengths, w_query, w_key, w_value, w_gate, state_in, log_gamma):
    batch_size, head_count, key_dim, value_dim = state_in.shape
    block_len = normed.shape[0] // batch_size
    queries = jnp.dot(normed, w_query, preferred_element_type=jnp.float32)
    queries = rotate(queries.reshape(batch_size, block_len, head_count, key_dim)).astype(jnp.bfloat16)
    key_rows = jnp.dot(normed, w_key, preferred_element_type=jnp.float32)
    key_rows = (rotate(key_rows.reshape(batch_size, block_len, head_count, key_dim)) * key_dim ** (-0.5)).astype(jnp.bfloat16)
    values = jnp.dot(normed, w_value, preferred_element_type=jnp.float32).astype(jnp.bfloat16)
    values = values.reshape(batch_size, block_len, head_count, value_dim)
    gate_pre = jnp.dot(normed, w_gate, preferred_element_type=jnp.float32).reshape(batch_size, block_len, head_count, value_dim)
    slot_ids = jnp.arange(block_len).astype(jnp.float32)
    live_count = lengths.astype(jnp.float32)
    active = (slot_ids[None, :] < live_count[:, None]).astype(jnp.float32)
    step_gap = slot_ids[:, None] - slot_ids[None, :]
    causal = (step_gap >= 0.0).astype(jnp.float32)
    within = jnp.exp(log_gamma[:, None, None] * jnp.maximum(step_gap, 0.0)[None]) * causal[None]
    scores = jnp.einsum('bihd,bjhd->bhij', queries.astype(jnp.float32), key_rows.astype(jnp.float32))
    weights = (scores * within[None]).astype(jnp.bfloat16)
    inner_part = jnp.einsum('bhij,bjhe->bihe', weights.astype(jnp.float32), values.astype(jnp.float32))
    carried = jnp.einsum('bihd,bhde->bihe', queries.astype(jnp.float32), state_in, precision=lax.Precision.HIGHEST)
    carried = carried * jnp.exp(log_gamma[None, None, :] * (slot_ids[None, :, None] + 1.0))[..., None]
    retained = (inner_part + carried) * active[:, :, None, None]
    lead_gap = live_count[:, None] - 1.0 - slot_ids[None, :]
    key_weight = jnp.exp(log_gamma[None, None, :] * jnp.maximum(lead_gap, 0.0)[:, :, None]) * active[:, :, None]
    added_state = jnp.einsum('bjhd,bjhe->bhde', key_rows.astype(jnp.float32) * key_weight[..., None], values.astype(jnp.float32), precision=lax.Precision.HIGHEST)
    new_state = state_in * jnp.exp(log_gamma[None, :] * live_count[:, None])[:, :, None, None] + added_state
    inv_rms = lax.rsqrt(lax.optimization_barrier(jnp.mean(retained * retained, axis=-1, keepdims=True)) + NORM_EPSILON)
    heads_out = (retained * inv_rms * jax.nn.silu(gate_pre)).astype(jnp.bfloat16)
    return (heads_out.reshape(batch_size * block_len, head_count * value_dim), new_state)

def one_block(stream, lengths, gain_vec, w_query, w_key, w_value, w_gate, w_out, state_in):
    normed = norm_rows(stream, gain_vec)
    log_gamma = decay_logs(state_in.shape[1])
    heads_out, new_state = retain(normed, lengths, w_query, w_key, w_value, w_gate, state_in, log_gamma)
    mix_rows = jnp.dot(heads_out, w_out, preferred_element_type=jnp.float32).astype(jnp.bfloat16)
    result = (stream.astype(jnp.float32) + mix_rows.astype(jnp.float32)).astype(jnp.bfloat16)
    return (result, new_state)

def reference(tokens, lengths, gain_first, query_first, key_first, value_first, gate_first, out_first, state_first, gain_second, query_second, key_second, value_second, gate_second, out_second, state_second):
    middle, state_first_new = one_block(tokens, lengths, gain_first, query_first, key_first, value_first, gate_first, out_first, state_first)
    mixed_out, state_second_new = one_block(middle, lengths, gain_second, query_second, key_second, value_second, gate_second, out_second, state_second)
    return (mixed_out, state_first_new, state_second_new)
```

```python
import functools

import jax
import jax.numpy as jnp
from jax import lax
from jax.experimental import pallas as pl
from jax.experimental.pallas import tpu as pltpu
from jax.sharding import PartitionSpec as P
import numpy as np

PAST_LEN = 16384
LIVE_TOTAL = 960

NORM_EPSILON = 1e-06
ROPE_BASE = 10000.0

MESH = pl.DeviceIdType.MESH
F32 = jnp.float32
BF16 = jnp.bfloat16


def decay_logs(head_count):
    head_total = lax.axis_size("tp") * head_count
    head_ids = (lax.axis_index("tp") * head_count + jnp.arange(head_count)).astype(F32)
    return jnp.log(1.0 - 2.0 ** (-1.5 - 6.0 * head_ids / (head_total - 1)))


def rope_tables(block_len, key_dim):
    half_dim = key_dim // 2
    inverse = ROPE_BASE ** (-jnp.arange(half_dim, dtype=F32) / half_dim)
    positions = PAST_LEN + jnp.arange(block_len, dtype=F32)
    angles = positions[:, None] * inverse[None, :]
    cosines, sines = jnp.cos(angles), jnp.sin(angles)
    cosines = jnp.concatenate([cosines, cosines], axis=1)
    sines = jnp.concatenate([-sines, sines], axis=1)
    scale = key_dim ** (-0.5)
    return jnp.concatenate([cosines, cosines * scale, sines, sines * scale], axis=1)


def retain(queries, key_rows, values, lengths, state_in):
    batch_size, head_count, key_dim, value_dim = state_in.shape
    block_len = queries.shape[0] // batch_size
    log_gamma = decay_logs(head_count)
    queries = queries.reshape(batch_size, block_len, head_count, key_dim)
    key_rows = key_rows.reshape(batch_size, block_len, head_count, key_dim)
    values = values.reshape(batch_size, block_len, head_count, value_dim)
    slot_ids = jnp.arange(block_len).astype(F32)
    live_count = lengths.astype(F32)
    active = (slot_ids[None, :] < live_count[:, None]).astype(F32)
    step_gap = slot_ids[:, None] - slot_ids[None, :]
    causal = (step_gap >= 0.0).astype(F32)
    within = jnp.exp(log_gamma[:, None, None] * jnp.maximum(step_gap, 0.0)[None]) * causal[None]
    scores = jnp.einsum("bihd,bjhd->bhij", queries, key_rows, preferred_element_type=F32)
    weights = (scores * within[None]).astype(BF16)
    inner_part = jnp.einsum("bhij,bjhe->bihe", weights, values, preferred_element_type=F32)
    carried = jnp.einsum(
        "bihd,bhde->bihe", queries.astype(F32), state_in, precision=lax.Precision.HIGHEST
    )
    carried = (
        carried * jnp.exp(log_gamma[None, None, :] * (slot_ids[None, :, None] + 1.0))[..., None]
    )
    retained = (inner_part + carried) * active[:, :, None, None]
    lead_gap = live_count[:, None] - 1.0 - slot_ids[None, :]
    key_weight = (
        jnp.exp(log_gamma[None, None, :] * jnp.maximum(lead_gap, 0.0)[:, :, None])
        * active[:, :, None]
    )
    added_state = jnp.einsum(
        "bjhd,bjhe->bhde",
        key_rows.astype(F32) * key_weight[..., None],
        values.astype(F32),
        precision=lax.Precision.HIGHEST,
    )
    new_state = (
        state_in * jnp.exp(log_gamma[None, :] * live_count[:, None])[:, :, None, None] + added_state
    )
    inv_rms = lax.rsqrt(jnp.mean(retained * retained, axis=-1, keepdims=True) + NORM_EPSILON)
    return (retained * inv_rms).reshape(batch_size * block_len, -1), new_state


def rotated(vectors, table, scale_at):
    key_dim = vectors.shape[-1]
    half = key_dim // 2
    swapped = jnp.concatenate([vectors[..., half:], vectors[..., :half]], axis=-1)
    cosines = table[:, None, scale_at * key_dim : (scale_at + 1) * key_dim]
    sines = table[:, None, (2 + scale_at) * key_dim : (3 + scale_at) * key_dim]
    return (vectors * cosines + swapped * sines).astype(BF16)


def plain_block(x, lengths, gain, qk_weights, w_value, w_gate, w_out, state, table):
    batch_size, head_count, key_dim, value_dim = state.shape
    whole = lax.all_gather(x, "tp", axis=1, tiled=True).astype(F32)
    inv = lax.rsqrt(jnp.mean(whole * whole, axis=-1, keepdims=True) + NORM_EPSILON)
    normed = (whole * inv * gain).astype(BF16)
    turned = []
    for scale_at, weight in enumerate(qk_weights):
        product = jnp.einsum("rd,dhk->rhk", normed, weight, preferred_element_type=F32)
        turned.append(rotated(product, table, scale_at))
    values = jnp.dot(normed, w_value, preferred_element_type=F32).astype(BF16)
    gate = jnp.dot(normed, w_gate, preferred_element_type=F32)
    retained, new_state = retain(turned[0], turned[1], values, lengths, state)
    heads_out = (retained * jax.nn.silu(gate)).astype(BF16)
    part = jnp.dot(heads_out, w_out, preferred_element_type=F32).astype(BF16)
    mix = lax.psum_scatter(part, "tp", scatter_dimension=1, tiled=True)
    return (x.astype(F32) + mix.astype(F32)).astype(BF16), new_state


FRONT = 32


class Plan:
    def __init__(self, n, rows, pieces, batch, block_len, key_dim, value_dim, width):
        self.n, self.m = n, n // 2
        self.rows, self.pieces, self.size = rows, pieces, rows // pieces
        self.batch, self.block_len = batch, block_len
        self.key_dim, self.value_dim, self.width = key_dim, value_dim, width
        self.slots = batch * block_len
        self.unit = 128
        self.units = self.slots // self.unit
        self.group = self.unit // block_len
        self.long = -(-(rows + FRONT) // 128) * 128
        half, quarter = pieces // 2, pieces // 4
        self.cw = [j for j in range(pieces) if j < quarter or j >= quarter + half]
        self.ccw = [j for j in range(pieces) if quarter <= j < quarter + half]
        self.blocks = [(0, quarter), (quarter, half), (half, quarter + half), (quarter + half, pieces)]
        self.order = [j for pair in zip(self.cw, self.ccw) for j in pair]

    def clockwise(self, j):
        return j in self.cw

    def piece(self, j):
        return pl.ds(j * self.size, self.size)

    def span(self, block):
        return pl.ds(block[0] * self.size, (block[1] - block[0]) * self.size)

    def first_sequence(self, row):
        return max(row // self.block_len, self.batch - self.rows + row)

    def last_sequence(self, row):
        return min(row, self.batch - -(-(self.rows - row) // self.block_len))


class Ring:
    def __init__(self, plan):
        self.plan, self.m = plan, plan.m
        me = lax.axis_index("tp")
        self.core = lax.rem(me, 2)
        chip = lax.div(me, 2)
        odd = lax.rem(chip, 2)
        half = lax.div(chip, 2)
        self.pos = (1 - odd) * half + odd * (self.m - 1 - half)
        self.me = me
        self.partner = chip * 2 + 1 - self.core
        self.right = self.device(self.pos + 1)
        self.left = self.device(self.pos - 1)

    def device(self, pos):
        m = self.m
        pos = lax.rem(pos + m, m)
        far = lax.div(pos, (m + 1) // 2)
        chip = (1 - far) * 2 * pos + far * (2 * (m - 1 - pos) + 1)
        return chip * 2 + self.core

    def greet(self):
        barrier = pltpu.get_barrier_semaphore()
        for device in (self.left, self.right, self.partner):
            pl.semaphore_signal(barrier, inc=1, device_id={"tp": device}, device_id_type=MESH)

    def met(self):
        pl.semaphore_wait(pltpu.get_barrier_semaphore(), 3)

    def to(self, j):
        return self.right if self.plan.clockwise(j) else self.left

    def origin(self, j, steps):
        back = self.pos - steps if self.plan.clockwise(j) else self.pos + steps
        return self.device(back)


def remote(src, dst, send, recv, device):
    return pltpu.make_async_remote_copy(
        src_ref=src,
        dst_ref=dst,
        send_sem=send,
        recv_sem=recv,
        device_id={"tp": device},
        device_id_type=MESH,
    )


def share_out(step, steps, total, work):
    per = -(-total // steps)
    for k in range(per):
        u = (step - 1) * per + k

        @pl.when(u < total)
        def _():
            work(u)


class Gather:
    def __init__(self, ring, own, whole, sems):
        self.ring, self.plan, self.own, self.whole = ring, ring.plan, own, whole
        self.send, self.recv, self.share_send, self.share_recv = sems

    def columns(self, device):
        return pl.ds(pl.multiple_of(device * self.plan.width, self.plan.width), self.plan.width)

    def place(self, j, s):
        return self.whole.at[self.plan.piece(j), self.columns(self.ring.origin(j, s))]

    def source(self, j, s):
        if isinstance(s, int) and s == 0:
            return self.own.at[self.plan.piece(j), :]
        return self.place(j, s)

    def hop(self, j, s):
        return remote(
            self.source(j, s), self.place(j, s), self.send.at[j, s], self.recv.at[j, s], self.ring.to(j)
        )

    def share(self, j, s):
        return remote(
            self.source(j, s),
            self.place(j, s),
            self.share_send.at[j, s],
            self.share_recv.at[j, s],
            self.ring.partner,
        )

    def begin(self, j):
        self.hop(j, 0).start()
        self.share(j, 0).start()
        self.whole[self.plan.piece(j), self.columns(self.ring.me)] = self.own[self.plan.piece(j), :]

    def forward(self, j, s, last):
        self.hop(j, s - 1).wait_recv()
        if not last:
            self.hop(j, s).start()
        self.share(j, s).start()

    def drain(self):
        for j in range(self.plan.pieces):
            self.hop(j, 0).wait_send()
            self.share(j, 0).wait_send()

        @pl.loop(1, self.plan.m - 1)
        def _(s):
            for j in range(self.plan.pieces):
                self.hop(j, s).wait_send()
                self.share(j, s).wait_send()

        for j in range(self.plan.pieces):
            self.share(j, self.plan.m - 1).wait_send()


class Projection:
    def __init__(self, gather, gain, wcat, total, squares):
        self.gather, self.plan, self.ring = gather, gather.plan, gather.ring
        self.gain, self.wcat, self.total, self.squares = gain, wcat, total, squares

    def product(self, block, s):
        plan = self.plan
        for j in range(*block):
            self.gather.share(j, s).wait_recv()
        chip = lax.div(self.ring.origin(block[0], s), 2)
        cols = pl.ds(pl.multiple_of(chip * 2 * plan.width, 2 * plan.width), 2 * plan.width)
        x = self.gather.whole[plan.span(block), cols].astype(F32)
        square = x * x
        part = square[:, :128]
        for k in range(128, 2 * plan.width, 128):
            part = part + square[:, k : k + 128]
        scaled = (x * self.gain[:, cols]).astype(BF16)
        return jnp.dot(scaled, self.wcat[cols, :], preferred_element_type=F32), part

    def first(self, block):
        at = self.plan.span(block)
        self.total[at, :], self.squares[at, :] = self.product(block, 0)

    def add(self, block, s):
        at = self.plan.span(block)
        product, part = self.product(block, s)
        self.total[at, :] += product
        self.squares[at, :] += part

    def finish(self, block, table, queries, kv, gate):
        plan = self.plan
        at = plan.span(block)
        product, part = self.product(block, plan.m - 1)
        square = self.squares[at, :] + part
        mean = jnp.sum(square, axis=-1, keepdims=True) / (plan.n * plan.width)
        out = (self.total[at, :] + product) * lax.rsqrt(mean + NORM_EPSILON)
        key_dim, both = plan.key_dim, 2 * plan.key_dim
        qk = out[:, :both]
        lane = lax.broadcasted_iota(jnp.int32, qk.shape, 1)
        ahead = pltpu.roll(qk, both - key_dim // 2, 1)
        behind = pltpu.roll(qk, key_dim // 2, 1)
        swapped = jnp.where(lax.rem(lane, key_dim) < key_dim // 2, ahead, behind)
        turned = qk * table[at, :both] + swapped * table[at, both:]
        crossed = pltpu.roll(turned, key_dim, 1)
        front = lane < key_dim
        queries[at, :] = jnp.where(front, turned, crossed).astype(BF16)
        low = pl.ds(FRONT + block[0] * plan.size, (block[1] - block[0]) * plan.size)
        kv[low, :both] = jnp.where(front, crossed, turned).astype(BF16)
        kv[low, both:] = out[:, both : both + plan.value_dim].astype(BF16)
        open_gate = out[:, both + plan.value_dim :]
        gate[at, :] = open_gate / (1.0 + jnp.exp(-open_gate))


def fill_unit(wq, wk, wcat, u):
    at = pl.ds(pl.multiple_of(u * 128, 128), 128)
    pair = jnp.concatenate([wq[:, at], wk[:, at]], axis=0)
    wcat[at, : 2 * wq.shape[0]] = jnp.transpose(pair.astype(F32)).astype(BF16)


def pack_rows(plan, lens_ref, tokens, x, trow, bounds, send):
    lens = jnp.broadcast_to(lens_ref[...].astype(F32), (8, plan.batch)).astype(BF16)
    wide = (plan.batch, plan.slots)
    sequence = lax.broadcasted_iota(jnp.int32, wide, 0)
    owner = lax.div(lax.broadcasted_iota(jnp.int32, wide, 1), plan.block_len)
    before = jnp.where(sequence < owner, 1.0, 0.0).astype(BF16)
    same = jnp.where(sequence == owner, 1.0, 0.0).astype(BF16)
    start = jnp.dot(lens, before, preferred_element_type=F32)
    count = jnp.dot(lens, same, preferred_element_type=F32)
    slot = lax.rem(lax.broadcasted_iota(jnp.int32, start.shape, 1), plan.block_len).astype(F32)
    trow[...] = jnp.where(slot < count, start + slot, -1.0)
    square = (plan.batch, plan.batch)
    earlier = lax.broadcasted_iota(jnp.int32, square, 0) < lax.broadcasted_iota(jnp.int32, square, 1)
    begin = jnp.dot(lens, jnp.where(earlier, 1.0, 0.0).astype(BF16), preferred_element_type=F32)
    bounds[0:8, :] = begin
    bounds[8:16, :] = begin + lens.astype(F32)
    base = lax.broadcasted_iota(jnp.int32, (plan.size, plan.slots), 0).astype(F32)
    for j in plan.order:
        hot = jnp.where(base + float(j * plan.size) == trow[0:1, :], 1.0, 0.0).astype(BF16)
        x[plan.piece(j), :] = jnp.dot(hot, tokens[...], preferred_element_type=F32).astype(BF16)
        send(j)


def row_unit(plan, bounds, rope, tcol, bcol, table, u):
    at = pl.ds(pl.multiple_of(u * plan.size, plan.size), plan.size)
    shape = (plan.size, plan.batch)
    row = (lax.broadcasted_iota(jnp.int32, shape, 0) + u * plan.size).astype(F32)
    begin, end = bounds[0:1, :], bounds[8:9, :]
    inside = (row >= begin) & (row < end)
    slot = jnp.sum(jnp.where(inside, row - begin, 0.0), axis=-1, keepdims=True)
    owner = jnp.sum(jnp.where(row >= end, 1.0, 0.0), axis=-1, keepdims=True)
    full = (plan.size, 128)
    slot = jnp.broadcast_to(slot, full)
    tcol[at, :] = slot
    bcol[at, :] = jnp.broadcast_to(owner, full).astype(BF16)
    lane = lax.broadcasted_iota(jnp.int32, full, 1)
    pick = (lax.rem(lane, plan.block_len).astype(F32) == slot) & (lane < 3 * plan.block_len)
    pick = jnp.where(pick, 1.0, 0.0).astype(BF16)
    table[at, :] = jnp.dot(pick, rope[...], preferred_element_type=F32)


def slot_unit(plan, rate, lens_ref, tgt, onward, hot, u):
    at = pl.ds(pl.multiple_of(u * plan.unit, plan.unit), plan.unit)
    lens = jnp.broadcast_to(lens_ref[...].astype(F32), (plan.unit, plan.batch)).astype(BF16)
    shape = (plan.unit, plan.batch)
    owner = lax.div(lax.broadcasted_iota(jnp.int32, shape, 0), plan.block_len) + u * plan.group
    sequence = lax.broadcasted_iota(jnp.int32, shape, 1)
    before = jnp.where(sequence < owner, 1.0, 0.0).astype(BF16)
    same = jnp.where(sequence == owner, 1.0, 0.0).astype(BF16)
    dims = (((1,), (1,)), ((), ()))
    start = lax.dot_general(before, lens, dims, preferred_element_type=F32)
    count = lax.dot_general(same, lens, dims, preferred_element_type=F32)
    full = (plan.unit, plan.unit)
    slot = lax.rem(lax.broadcasted_iota(jnp.int32, full, 0), plan.block_len).astype(F32)
    target = jnp.where(slot < count, start + slot, -1.0)
    tgt[at, :] = target
    onward[at, :] = jnp.exp(rate * jnp.maximum(count - 1.0 - slot, 0.0))
    moved = jnp.where(target >= 0.0, target + float(FRONT), -1.0)
    lane = lax.broadcasted_iota(jnp.int32, full, 1).astype(F32)
    for c in range(plan.long // 128):
        hot[at, c * 128 : (c + 1) * 128] = jnp.where(moved == lane + float(c * 128), 1.0, 0.0).astype(BF16)


def split_unit(plan, state, halves, u):
    at = pl.ds(pl.multiple_of(u * plan.group, plan.group), plan.group)
    rows = plan.group * plan.key_dim
    whole = state[at].reshape(rows, plan.value_dim)
    high = whole.astype(BF16)
    to = pl.ds(pl.multiple_of(u * rows, rows), rows)
    halves[to, : plan.value_dim] = high
    halves[to, plan.value_dim :] = (whole - high.astype(F32)).astype(BF16)


def state_unit(plan, lens_smem, powers, me, hot, kv, onward, state, u):
    at = pl.ds(pl.multiple_of(u * plan.unit, plan.unit), plan.unit)
    both = 2 * plan.key_dim
    padded = jnp.dot(hot[at, :], kv[...], preferred_element_type=F32)
    values = padded[:, both:].astype(BF16)
    scaled = padded[:, :both] * onward[at, :]
    high = scaled.astype(BF16).astype(F32)
    wide = (plan.unit, plan.group * plan.key_dim)
    own = lax.div(lax.broadcasted_iota(jnp.int32, wide, 0), plan.block_len) == lax.div(
        lax.broadcasted_iota(jnp.int32, wide, 1), plan.key_dim
    )
    added = None
    for piece in (high, scaled - high):
        spread = jnp.where(own, jnp.concatenate([piece] * (plan.group // 2), axis=1), 0.0)
        term = lax.dot_general(
            spread.astype(BF16), values, (((0,), (0,)), ((), ())), preferred_element_type=F32
        )
        added = term if added is None else added + term
    for b in range(plan.group):
        which = u * plan.group + b
        decay = powers[me, lens_smem[which]]
        state[which] = state[which] * decay + added[b * plan.key_dim : (b + 1) * plan.key_dim, :]


def retention_block(plan, rate, block, queries, kv, gate, tcol, bcol, fade, halves):
    both = 2 * plan.key_dim
    inner = []
    shape = (plan.size, 128)
    gap = lax.broadcasted_iota(jnp.int32, shape, 0) - lax.broadcasted_iota(jnp.int32, shape, 1)
    gap = (gap + FRONT).astype(F32)
    for j in range(*block):
        window = pl.ds(j * plan.size, 128)
        scores = lax.dot_general(
            queries[plan.piece(j), :],
            kv[window, :both],
            (((1,), (1,)), ((), ())),
            preferred_element_type=F32,
        )
        weights = jnp.where(gap <= tcol[plan.piece(j), :], scores * fade[...], 0.0).astype(BF16)
        inner.append(jnp.dot(weights, kv[window, both:], preferred_element_type=F32))
    at = plan.span(block)
    low = plan.first_sequence(block[0] * plan.size) // 2
    high = plan.last_sequence(block[1] * plan.size - 1) // 2 + 1
    q, owner = queries[at, :], bcol[at, :]
    lane = lax.broadcasted_iota(jnp.int32, (q.shape[0], both), 1)
    pick = owner - jnp.where(lane < plan.key_dim, 0.0, 1.0).astype(BF16)
    zero = jnp.zeros_like(q)
    spread = [jnp.where(pick == jnp.asarray(2.0 * c, BF16), q, zero) for c in range(low, high)]
    carried = jnp.dot(
        jnp.concatenate(spread, axis=1),
        halves[low * both : high * both, :],
        preferred_element_type=F32,
    )
    carried = carried[:, : plan.value_dim] + carried[:, plan.value_dim :]
    retained = jnp.concatenate(inner, axis=0) + carried * jnp.exp(rate * (tcol[at, :] + 1.0))
    inv = lax.rsqrt(jnp.mean(retained * retained, axis=-1, keepdims=True) + NORM_EPSILON)
    return (retained * inv * gate[at, :]).astype(BF16)


class Scatter:
    def __init__(self, ring, h_pair, w_pair, outbox, inbox, parts, sems):
        self.ring, self.plan = ring, ring.plan
        self.h_pair, self.w_pair, self.outbox, self.inbox, self.parts = h_pair, w_pair, outbox, inbox, parts
        self.send, self.recv, self.pair_send, self.pair_recv = sems

    def offer(self, k):
        rows, depth = self.plan.span(self.plan.blocks[k]), self.plan.value_dim
        return remote(
            self.h_pair.at[rows, pl.ds(0, depth)],
            self.h_pair.at[rows, pl.ds(depth, depth)],
            self.pair_send.at[k],
            self.pair_recv.at[k],
            self.ring.partner,
        )

    def hop(self, j, s):
        return remote(
            self.outbox.at[j, s],
            self.inbox.at[j, s],
            self.send.at[j, s],
            self.recv.at[j, s],
            self.ring.to(j),
        )

    def product(self, k, s):
        block, width = self.plan.blocks[k], self.plan.width
        target = self.ring.origin(block[0], s + 1)
        cols = pl.ds(pl.multiple_of(target * width, width), width)
        return jnp.dot(
            self.h_pair[self.plan.span(block), :], self.w_pair[:, cols], preferred_element_type=F32
        )

    def begin(self, k):
        self.offer(k).wait_recv()
        part = self.product(k, 0).astype(BF16)
        first, last = self.plan.blocks[k]
        for j in range(first, last):
            self.outbox[j, 0] = part[(j - first) * self.plan.size : (j - first + 1) * self.plan.size, :]
            self.hop(j, 0).start()

    def prepare(self, k, s):
        self.parts[lax.rem(s, 2), self.plan.span(self.plan.blocks[k]), :] = self.product(k, s)

    def take(self, j, s):
        self.hop(j, s - 1).wait_recv()
        return self.parts[lax.rem(s, 2), self.plan.piece(j), :] + self.inbox[j, s - 1].astype(F32)

    def forward(self, j, s):
        self.outbox[j, s] = self.take(j, s).astype(BF16)
        self.hop(j, s).start()

    def steps(self, work):
        for k in range(4):
            self.prepare(k, 1)

        @pl.loop(1, self.plan.m - 1)
        def _(s):
            for i, j in enumerate(self.plan.order):
                self.forward(j, s)
                if i % 2 == 1 and i < 8:
                    self.prepare(i // 2, s + 1)
            for i in range(len(self.plan.order) // 2, 4):
                self.prepare(i, s + 1)
            work(s)

    def last(self, j):
        return self.take(j, self.plan.m - 1).astype(BF16).astype(F32)

    def drain(self):
        for k in range(4):
            self.offer(k).wait_send()

        @pl.loop(0, self.plan.m - 1)
        def _(s):
            for j in range(self.plan.pieces):
                self.hop(j, s).wait_send()


def whole_kernel(plan, *refs):
    (lens_smem, powers, rates, lens_ref, tokens, rope, *rest) = refs
    gains, raw, outs_w, states_in, (mixed, *states_out), scratch = (
        (rest[0], rest[7]),
        (rest[1:5], rest[8:12]),
        (rest[5], rest[12]),
        (rest[6], rest[13]),
        rest[14:17],
        rest[17:],
    )
    (x, x1, y, whole, wcats, turned, w_pairs, total, squares, table, gate, tcol, bcol, queries) = scratch[:14]
    (kv, halves, states, hot, onward, tgt, parts, outbox, inbox, h_pair, trow, bounds, fade) = scratch[14:27]
    load, store, pair_w = scratch[27:30]
    sems = scratch[30:]
    ring = Ring(plan)
    ring.greet()
    depth, both = plan.value_dim, 2 * plan.key_dim
    rate = rates[0, ring.me]

    loads = {}
    for i in range(2):
        wq, wk, wv, wg = raw[i]
        targets = (
            (wq, turned.at[i, 0]),
            (wk, turned.at[i, 1]),
            (wv, wcats.at[i, :, pl.ds(both, depth)]),
            (wg, wcats.at[i, :, pl.ds(both + depth, depth)]),
            (outs_w[i], w_pairs.at[i, pl.ds(0, depth), :]),
            (states_in[i], states.at[i]),
        )
        for k, (source, target) in enumerate(targets):
            loads[i, k] = pltpu.make_async_copy(source, target, load.at[i, k])

    def swap(i):
        return remote(
            w_pairs.at[i, pl.ds(0, depth), :],
            w_pairs.at[i, pl.ds(depth, depth), :],
            pair_w.at[0, i],
            pair_w.at[1, i],
            ring.partner,
        )

    gathers = [Gather(ring, (x, x1)[i], whole, sems[8 * i : 8 * i + 4]) for i in range(2)]
    scatters = [
        Scatter(ring, h_pair, w_pairs.at[i], outbox, inbox, parts, sems[8 * i + 4 : 8 * i + 8])
        for i in range(2)
    ]
    projections = [Projection(gathers[i], gains[i], wcats.at[i], total, squares) for i in range(2)]

    for k in range(6):
        loads[0, k].start()
    met = []

    def send(j):
        if not met:
            ring.met()
            met.append(1)
        gathers[0].begin(j)

    pack_rows(plan, lens_ref, tokens, x, trow, bounds, send)
    for k in range(6):
        loads[1, k].start()
    loads[0, 0].wait()
    loads[0, 1].wait()

    @pl.loop(0, wcats.shape[1] // 128)
    def _(u):
        fill_unit(turned.at[0, 0], turned.at[0, 1], wcats.at[0], u)

    loads[0, 2].wait()
    loads[0, 3].wait()
    shape = (plan.size, 128)
    gap = lax.broadcasted_iota(jnp.int32, shape, 0) - lax.broadcasted_iota(jnp.int32, shape, 1)
    gap = (gap + FRONT).astype(F32)
    near = (gap >= 0.0) & (gap < float(plan.block_len))
    fade[...] = jnp.where(near, 0.5 * jnp.exp(rate * jnp.maximum(gap, 0.0)), 0.0)
    kv[:FRONT, :] = jnp.zeros((FRONT, kv.shape[1]), BF16)
    kv[FRONT + plan.rows :, :] = jnp.zeros((plan.long - FRONT - plan.rows, kv.shape[1]), BF16)
    y[:FRONT, :] = jnp.zeros((FRONT, plan.width), BF16)
    y[FRONT + plan.rows :, :] = jnp.zeros((plan.long - FRONT - plan.rows, plan.width), BF16)
    loads[0, 5].wait()
    loads[0, 4].wait()
    swap(0).start()

    def run(i, gather_work, before_last, scatter_work, finish):
        gather, projection, scatter = gathers[i], projections[i], scatters[i]
        m, blocks = plan.m, plan.blocks

        def gather_step(s, last):
            for k, j in enumerate(plan.order):
                gather.forward(j, s, last)
                if k % 2 == 1 and k < 8:
                    if isinstance(s, int) and s == 1:
                        projection.first(blocks[k // 2])
                    else:
                        projection.add(blocks[k // 2], s - 1)
            for k in range(len(plan.order) // 2, 4):
                if isinstance(s, int) and s == 1:
                    projection.first(blocks[k])
                else:
                    projection.add(blocks[k], s - 1)

        gather_step(1, False)
        gather_work(1)

        @pl.loop(2, m - 1)
        def _(s):
            gather_step(s, False)
            gather_work(s)

        gather_step(m - 1, True)
        before_last()
        gather.drain()

        def retain_block(k):
            block = blocks[k]
            projection.finish(block, table, queries, kv, gate)
            h_pair[plan.span(block), :depth] = retention_block(
                plan, rate, block, queries, kv, gate, tcol, bcol, fade, halves
            )
            scatter.offer(k).start()

        retain_block(0)
        retain_block(1)
        swap(i).wait_recv()
        scatter.begin(0)
        retain_block(2)
        scatter.begin(1)
        retain_block(3)
        scatter.begin(2)
        scatter.begin(3)
        scatter.steps(scatter_work)
        for j in plan.order:
            finish(j, scatter.last(j))
        scatter.drain()
        swap(i).wait_send()

    def first_gather(s):
        share_out(s, plan.m - 2, plan.pieces, lambda u: row_unit(plan, bounds, rope, tcol, bcol, table, u))
        share_out(s, plan.m - 2, plan.units, lambda u: split_unit(plan, states.at[0], halves, u))
        share_out(
            s, plan.m - 2, plan.units, lambda u: slot_unit(plan, rate, lens_ref, tgt, onward, hot, u)
        )

    def update(i, s):
        share_out(
            s,
            plan.m - 2,
            plan.units,
            lambda u: state_unit(plan, lens_smem, powers, ring.me, hot, kv, onward, states.at[i], u),
        )

    def first_scatter(s):
        update(0, s)

    def after_first(j, mix):
        at = plan.piece(j)
        x1[at, :] = (x[at, :].astype(F32) + mix).astype(BF16)
        gathers[1].begin(j)

    run(0, first_gather, lambda: None, first_scatter, after_first)
    save = pltpu.make_async_copy(states.at[0], states_out[0], store.at[0])
    save.start()
    for k in range(6):
        loads[1, k].wait()
    swap(1).start()

    @pl.loop(0, wcats.shape[1] // 128)
    def _(u):
        fill_unit(turned.at[1, 0], turned.at[1, 1], wcats.at[1], u)

    def second_gather(s):
        share_out(s, plan.m - 2, plan.units, lambda u: split_unit(plan, states.at[1], halves, u))

    def after_second(j, mix):
        at = plan.piece(j)
        y[pl.ds(FRONT + j * plan.size, plan.size), :] = (x1[at, :].astype(F32) + mix).astype(BF16)

    run(1, second_gather, lambda: None, lambda s: update(1, s), after_second)
    save_second = pltpu.make_async_copy(states.at[1], states_out[1], store.at[1])
    save_second.start()
    many = next(k for k in (3, 2, 1) if plan.units % k == 0)

    @pl.loop(0, plan.units // many)
    def _(u):
        at = pl.ds(pl.multiple_of(u * many * plan.unit, plan.unit), many * plan.unit)
        spread = jnp.dot(hot[at, :], y[...], preferred_element_type=F32)
        live = jnp.concatenate([tgt[at, :]] * (plan.width // 128), axis=1) >= 0.0
        mixed[at, :] = jnp.where(live, spread, tokens[at, :].astype(F32)).astype(BF16)

    save.wait()
    save_second.wait()


def fused(plan, heads, lengths, tokens, first, second):
    total_heads = heads
    logs = np.log(1.0 - 2.0 ** (-1.5 - 6.0 * np.arange(total_heads) / (total_heads - 1)))
    powers = np.exp(logs[:, None] * np.arange(plan.block_len + 1)[None, :]).astype(np.float32)
    half = plan.key_dim // 2
    inverse = np.float32(ROPE_BASE) ** (-np.arange(half, dtype=np.float32) / np.float32(half))
    positions = PAST_LEN + np.arange(plan.block_len, dtype=np.float32)
    angles = (positions[:, None] * inverse.astype(np.float32)[None, :]).astype(np.float64)
    cosines, sines = np.cos(angles), np.sin(angles)
    cosines = np.concatenate([cosines, cosines], axis=1)
    sines = np.concatenate([-sines, sines], axis=1)
    scale = plan.key_dim**-0.5
    rope = np.concatenate([cosines, cosines * scale, sines, sines * scale], axis=1).astype(np.float32)
    stacked, rest = [], rope
    for _ in range(3):
        stacked.append(rest.astype(jnp.bfloat16))
        rest = rest - stacked[-1].astype(np.float32)
    rope = np.zeros((128, rope.shape[1]), jnp.bfloat16)
    rope[: 3 * plan.block_len] = np.concatenate(stacked, axis=0)

    n, m, rows, width = plan.n, plan.m, plan.rows, plan.width
    wide, both = 2 * plan.key_dim + 2 * plan.value_dim, 2 * plan.key_dim
    depth = plan.value_dim
    model = n * width
    state_shape = (plan.batch, plan.key_dim, plan.value_dim)
    vmem = lambda shape, kind: pltpu.VMEM(shape, kind)
    dma = lambda *shape: pltpu.SemaphoreType.DMA(shape)
    scratch = [
        vmem((rows, width), BF16),
        vmem((rows, width), BF16),
        vmem((plan.long, width), BF16),
        vmem((rows, model), BF16),
        vmem((2, model, wide), BF16),
        vmem((2, 2, plan.key_dim, model), BF16),
        vmem((2, 2 * depth, model), BF16),
        vmem((rows, wide), F32),
        vmem((rows, 128), F32),
        vmem((rows, 2 * both), F32),
        vmem((rows, depth), F32),
        vmem((rows, 128), F32),
        vmem((rows, 128), BF16),
        vmem((rows, both), BF16),
        vmem((plan.long, both + depth), BF16),
        vmem((plan.batch * plan.key_dim, 2 * depth), BF16),
        vmem((2,) + state_shape, F32),
        vmem((plan.slots, plan.long), BF16),
        vmem((plan.slots, 128), F32),
        vmem((plan.slots, 128), F32),
        vmem((2, rows, width), F32),
        vmem((plan.pieces, m - 1, plan.size, width), BF16),
        vmem((plan.pieces, m - 1, plan.size, width), BF16),
        vmem((rows, 2 * depth), BF16),
        vmem((8, plan.slots), F32),
        vmem((16, plan.batch), F32),
        vmem((plan.size, 128), F32),
        dma(2, 6),
        dma(2),
        dma(2, 2),
    ]
    for _ in range(2):
        scratch += [dma(plan.pieces, m - 1)] * 2 + [dma(plan.pieces, m)] * 2
        scratch += [dma(plan.pieces, m - 1)] * 2 + [dma(4)] * 2
    spec = lambda space: pl.BlockSpec(memory_space=space)
    inside, outside, scalars = spec(pltpu.VMEM), spec(pltpu.HBM), spec(pltpu.SMEM)

    def group(gain, query, key, value, gate, out, state):
        return (gain[None], query.T, key.T, value, gate, out, state.reshape(state_shape))

    block_specs = [inside] + [outside] * 6
    mixed, one, two = pl.pallas_call(
        functools.partial(whole_kernel, plan),
        out_shape=[
            jax.ShapeDtypeStruct((plan.slots, width), BF16),
            jax.ShapeDtypeStruct(state_shape, F32),
            jax.ShapeDtypeStruct(state_shape, F32),
        ],
        in_specs=[scalars] * 3 + [inside] * 3 + block_specs * 2,
        out_specs=[inside, outside, outside],
        scratch_shapes=scratch,
        compiler_params=pltpu.CompilerParams(
            collective_id=0, has_side_effects=True, vmem_limit_bytes=62 * 2**20
        ),
    )(
        lengths,
        jnp.asarray(powers),
        jnp.asarray(logs.astype(np.float32)[None, :]),
        lengths[None, :],
        tokens,
        jnp.asarray(rope),
        *group(*first),
        *group(*second),
    )
    return mixed, one.reshape(first[-1].shape), two.reshape(second[-1].shape)


def unpacked(lengths, tokens, first, second):
    batch_size, head_count, key_dim, value_dim = first[-1].shape
    slots = tokens.shape[0]
    block_len = slots // batch_size
    table = jnp.tile(rope_tables(block_len, key_dim), (batch_size, 1))
    x, states = tokens, []
    for gain, query, key, value, gate, out, state in (first, second):
        qk = []
        for weight in (query, key):
            qk.append(weight.reshape(weight.shape[0], head_count, key_dim))
        x, new_state = plain_block(x, lengths, gain, qk, value, gate, out, state, table)
        states.append(new_state)
    return (x, *states)


def shards(
    tokens,
    lengths,
    gain_first,
    query_first,
    key_first,
    value_first,
    gate_first,
    out_first,
    state_first,
    gain_second,
    query_second,
    key_second,
    value_second,
    gate_second,
    out_second,
    state_second,
):
    n = lax.axis_size("tp")
    batch_size, head_count, key_dim, value_dim = state_first.shape
    slots, width = tokens.shape
    block_len = slots // batch_size
    rows = LIVE_TOTAL
    lengths = lengths.astype(jnp.int32)
    first = (gain_first, query_first, key_first, value_first, gate_first, out_first, state_first)
    second = (gain_second, query_second, key_second, value_second, gate_second, out_second, state_second)
    pieces = next((p for p in (10, 8, 6, 4) if rows % (16 * p) == 0 and rows // p <= 128 - FRONT), 0)
    fits = (
        n >= 8
        and n % 2 == 0
        and pieces > 0
        and head_count == 1
        and width == 128
        and value_dim == 128
        and key_dim == 64
        and block_len <= FRONT
        and 128 % (2 * block_len) == 0
        and 3 * block_len <= 128
        and batch_size <= 128
        and batch_size % 2 == 0
        and slots % 128 == 0
    )
    if not fits:
        return unpacked(lengths, tokens, first, second)
    plan = Plan(n, rows, pieces, batch_size, block_len, key_dim, value_dim, width)
    return fused(plan, n * head_count, lengths, tokens, first, second)


def solution(mesh):
    heads = P(None, "tp")
    state = P("grp", "tp", None, None)
    block = (P(), heads, heads, heads, heads, P("tp", None), state)
    in_specs = (P("grp", "tp"), P("grp")) + block + block
    out_specs = (P("grp", "tp"), state, state)
    return jax.shard_map(shards, mesh=mesh, in_specs=in_specs, out_specs=out_specs, check_vma=False)
```

```python
import functools

import jax
import jax.numpy as jnp
from jax import lax
from jax.experimental import pallas as pl
from jax.experimental.pallas import tpu as pltpu
from jax.sharding import PartitionSpec as P
import numpy as np

PAST_LEN = 16384
LIVE_TOTAL = 960

NORM_EPSILON = 1e-06
ROPE_BASE = 10000.0

MESH = pl.DeviceIdType.MESH
F32 = jnp.float32
BF16 = jnp.bfloat16


def decay_logs(head_count):
    head_total = lax.axis_size("tp") * head_count
    head_ids = (lax.axis_index("tp") * head_count + jnp.arange(head_count)).astype(F32)
    return jnp.log(1.0 - 2.0 ** (-1.5 - 6.0 * head_ids / (head_total - 1)))


def rope_tables(block_len, key_dim):
    half_dim = key_dim // 2
    inverse = ROPE_BASE ** (-jnp.arange(half_dim, dtype=F32) / half_dim)
    positions = PAST_LEN + jnp.arange(block_len, dtype=F32)
    angles = positions[:, None] * inverse[None, :]
    cosines, sines = jnp.cos(angles), jnp.sin(angles)
    cosines = jnp.concatenate([cosines, cosines], axis=1)
    sines = jnp.concatenate([-sines, sines], axis=1)
    scale = key_dim ** (-0.5)
    return jnp.concatenate([cosines, cosines * scale, sines, sines * scale], axis=1)


def retain(queries, key_rows, values, lengths, state_in):
    batch_size, head_count, key_dim, value_dim = state_in.shape
    block_len = queries.shape[0] // batch_size
    log_gamma = decay_logs(head_count)
    queries = queries.reshape(batch_size, block_len, head_count, key_dim)
    key_rows = key_rows.reshape(batch_size, block_len, head_count, key_dim)
    values = values.reshape(batch_size, block_len, head_count, value_dim)
    slot_ids = jnp.arange(block_len).astype(F32)
    live_count = lengths.astype(F32)
    active = (slot_ids[None, :] < live_count[:, None]).astype(F32)
    step_gap = slot_ids[:, None] - slot_ids[None, :]
    causal = (step_gap >= 0.0).astype(F32)
    within = jnp.exp(log_gamma[:, None, None] * jnp.maximum(step_gap, 0.0)[None]) * causal[None]
    scores = jnp.einsum("bihd,bjhd->bhij", queries, key_rows, preferred_element_type=F32)
    weights = (scores * within[None]).astype(BF16)
    inner_part = jnp.einsum("bhij,bjhe->bihe", weights, values, preferred_element_type=F32)
    carried = jnp.einsum(
        "bihd,bhde->bihe", queries.astype(F32), state_in, precision=lax.Precision.HIGHEST
    )
    carried = (
        carried * jnp.exp(log_gamma[None, None, :] * (slot_ids[None, :, None] + 1.0))[..., None]
    )
    retained = (inner_part + carried) * active[:, :, None, None]
    lead_gap = live_count[:, None] - 1.0 - slot_ids[None, :]
    key_weight = (
        jnp.exp(log_gamma[None, None, :] * jnp.maximum(lead_gap, 0.0)[:, :, None])
        * active[:, :, None]
    )
    added_state = jnp.einsum(
        "bjhd,bjhe->bhde",
        key_rows.astype(F32) * key_weight[..., None],
        values.astype(F32),
        precision=lax.Precision.HIGHEST,
    )
    new_state = (
        state_in * jnp.exp(log_gamma[None, :] * live_count[:, None])[:, :, None, None] + added_state
    )
    inv_rms = lax.rsqrt(jnp.mean(retained * retained, axis=-1, keepdims=True) + NORM_EPSILON)
    return (retained * inv_rms).reshape(batch_size * block_len, -1), new_state


def rotated(vectors, table, scale_at):
    key_dim = vectors.shape[-1]
    half = key_dim // 2
    swapped = jnp.concatenate([vectors[..., half:], vectors[..., :half]], axis=-1)
    cosines = table[:, None, scale_at * key_dim : (scale_at + 1) * key_dim]
    sines = table[:, None, (2 + scale_at) * key_dim : (3 + scale_at) * key_dim]
    return (vectors * cosines + swapped * sines).astype(BF16)


def plain_block(x, lengths, gain, qk_weights, w_value, w_gate, w_out, state, table):
    batch_size, head_count, key_dim, value_dim = state.shape
    whole = lax.all_gather(x, "tp", axis=1, tiled=True).astype(F32)
    inv = lax.rsqrt(jnp.mean(whole * whole, axis=-1, keepdims=True) + NORM_EPSILON)
    normed = (whole * inv * gain).astype(BF16)
    turned = []
    for scale_at, weight in enumerate(qk_weights):
        product = jnp.einsum("rd,dhk->rhk", normed, weight, preferred_element_type=F32)
        turned.append(rotated(product, table, scale_at))
    values = jnp.dot(normed, w_value, preferred_element_type=F32).astype(BF16)
    gate = jnp.dot(normed, w_gate, preferred_element_type=F32)
    retained, new_state = retain(turned[0], turned[1], values, lengths, state)
    heads_out = (retained * jax.nn.silu(gate)).astype(BF16)
    part = jnp.dot(heads_out, w_out, preferred_element_type=F32).astype(BF16)
    mix = lax.psum_scatter(part, "tp", scatter_dimension=1, tiled=True)
    return (x.astype(F32) + mix.astype(F32)).astype(BF16), new_state


FRONT = 32


class Plan:
    def __init__(self, n, rows, pieces, batch, block_len, key_dim, value_dim, width):
        self.n, self.m, self.far = n, n // 2, n // 4
        self.rows, self.pieces, self.size = rows, pieces, rows // pieces
        self.batch, self.block_len = batch, block_len
        self.key_dim, self.value_dim, self.width = key_dim, value_dim, width
        self.slots = batch * block_len
        self.unit = 128
        self.units = self.slots // self.unit
        self.group = self.unit // block_len
        self.long = -(-(rows + FRONT) // 128) * 128
        self.blocks = [(j, j + 2) for j in range(0, pieces, 2)]

    def reach(self, j, way):
        return self.far if j % 2 == way else self.far - 1

    def piece(self, j):
        return pl.ds(j * self.size, self.size)

    def span(self, block):
        return pl.ds(block[0] * self.size, (block[1] - block[0]) * self.size)

    def first_sequence(self, row):
        return max(row // self.block_len, self.batch - self.rows + row)

    def last_sequence(self, row):
        return min(row, self.batch - -(-(self.rows - row) // self.block_len))


class Ring:
    def __init__(self, plan):
        self.plan, self.m = plan, plan.m
        me = lax.axis_index("tp")
        self.core = lax.rem(me, 2)
        chip = lax.div(me, 2)
        odd = lax.rem(chip, 2)
        half = lax.div(chip, 2)
        self.pos = (1 - odd) * half + odd * (self.m - 1 - half)
        self.me = me
        self.partner = chip * 2 + 1 - self.core
        self.next = (self.device(self.pos + 1), self.device(self.pos - 1))

    def device(self, pos):
        m = self.m
        pos = lax.rem(pos + m, m)
        far = lax.div(pos, m // 2)
        chip = (1 - far) * 2 * pos + far * (2 * (m - 1 - pos) + 1)
        return chip * 2 + self.core

    def greet(self):
        barrier = pltpu.get_barrier_semaphore()
        for device in (*self.next, self.partner):
            pl.semaphore_signal(barrier, inc=1, device_id={"tp": device}, device_id_type=MESH)

    def met(self):
        pl.semaphore_wait(pltpu.get_barrier_semaphore(), 3)

    def behind(self, way, steps):
        return self.device(self.pos - steps if way == 0 else self.pos + steps)

    def ahead(self, way, steps):
        return self.device(self.pos + steps if way == 0 else self.pos - steps)


def remote(src, dst, send, recv, device):
    return pltpu.make_async_remote_copy(
        src_ref=src,
        dst_ref=dst,
        send_sem=send,
        recv_sem=recv,
        device_id={"tp": device},
        device_id_type=MESH,
    )


class Gather:
    def __init__(self, ring, own, whole, sems):
        self.ring, self.plan, self.own, self.whole = ring, ring.plan, own, whole
        self.out, self.recv, self.share_recv = sems

    def columns(self, device):
        return pl.ds(pl.multiple_of(device * self.plan.width, self.plan.width), self.plan.width)

    def place(self, j, way, h):
        return self.whole.at[self.plan.piece(j), self.columns(self.ring.behind(way, h))]

    def source(self, j, way, h):
        return self.own.at[self.plan.piece(j), :] if h == 0 else self.place(j, way, h)

    def hop(self, j, way, h):
        return remote(
            self.source(j, way, h - 1),
            self.place(j, way, h - 1),
            self.out.at[0],
            self.recv.at[j, way, h - 1],
            self.ring.next[way],
        )

    def share(self, j, way, h):
        return remote(
            self.source(j, way, h),
            self.place(j, way, h),
            self.out.at[1],
            self.share_recv.at[j // 2, h],
            self.ring.partner,
        )

    def begin(self, j):
        for way in (0, 1):
            self.hop(j, way, 1).start()
        self.share(j, 0, 0).start()
        self.whole[self.plan.piece(j), self.columns(self.ring.me)] = self.own[self.plan.piece(j), :]

    def arrive(self, j, way, h):
        reach = self.plan.reach(j, way)
        if h > reach:
            return
        self.hop(j, way, h).wait_recv()
        if h < reach:
            self.hop(j, way, h + 1).start()
        self.share(j, way, h).start()

    def shared(self, k, h):
        wide = self.plan.width if h in (0, self.plan.far) else 2 * self.plan.width
        every = self.whole.at[self.plan.span(self.plan.blocks[k]), pl.ds(0, wide)]
        remote(every, every, self.out.at[1], self.share_recv.at[k, h], self.ring.partner).wait_recv()

    def drain(self):
        for k, count in enumerate((self.plan.m - 1, self.plan.m)):
            every = self.whole.at[:, pl.ds(0, count * self.plan.width)]
            remote(every, every, self.out.at[k], self.share_recv.at[0, 0], self.ring.partner).wait_send()


class Projection:
    def __init__(self, gather, gain, wcat, total, squares):
        self.gather, self.plan, self.ring = gather, gather.plan, gather.ring
        self.gain, self.wcat, self.total, self.squares = gain, wcat, total, squares

    def product(self, at, h):
        plan = self.plan
        product, part = None, None
        for way in (0, 1) if 0 < h < plan.far else (0,):
            chip = lax.div(self.ring.behind(way, h), 2)
            cols = pl.ds(pl.multiple_of(chip * 2 * plan.width, 2 * plan.width), 2 * plan.width)
            x = self.gather.whole[at, cols].astype(F32)
            square = x * x
            for k in range(0, 2 * plan.width, 128):
                part = square[:, k : k + 128] if part is None else part + square[:, k : k + 128]
            scaled = (x * self.gain[:, cols]).astype(BF16)
            term = jnp.dot(scaled, self.wcat[cols, :], preferred_element_type=F32)
            product = term if product is None else product + term
        return product, part

    def add(self, k, h):
        plan = self.plan
        block = plan.blocks[k]
        self.gather.shared(k, h)
        at = plan.span(block)
        product, part = self.product(at, h)
        if h == 0:
            self.total[at, :], self.squares[at, :] = product, part
        else:
            self.total[at, :] += product
            self.squares[at, :] += part

    def finish(self, block, table, queries, kv, gate):
        plan = self.plan
        at = plan.span(block)
        self.gather.shared(plan.blocks.index(block), plan.far)
        product, part = self.product(at, plan.far)
        square = self.squares[at, :] + part
        mean = jnp.sum(square, axis=-1, keepdims=True) / (plan.n * plan.width)
        out = (self.total[at, :] + product) * lax.rsqrt(mean + NORM_EPSILON)
        key_dim, both = plan.key_dim, 2 * plan.key_dim
        qk = out[:, :both]
        lane = lax.broadcasted_iota(jnp.int32, qk.shape, 1)
        ahead = pltpu.roll(qk, both - key_dim // 2, 1)
        behind = pltpu.roll(qk, key_dim // 2, 1)
        swapped = jnp.where(lax.rem(lane, key_dim) < key_dim // 2, ahead, behind)
        turned = qk * table[at, :both] + swapped * table[at, both:]
        crossed = pltpu.roll(turned, key_dim, 1)
        front = lane < key_dim
        queries[at, :] = jnp.where(front, turned, crossed).astype(BF16)
        low = pl.ds(FRONT + block[0] * plan.size, (block[1] - block[0]) * plan.size)
        kv[low, :both] = jnp.where(front, crossed, turned).astype(BF16)
        kv[low, both:] = out[:, both : both + plan.value_dim].astype(BF16)
        open_gate = out[:, both + plan.value_dim :]
        gate[at, :] = open_gate / (1.0 + jnp.exp(-open_gate))


def fill_unit(wq, wk, wcat, u):
    at = pl.ds(pl.multiple_of(u * 128, 128), 128)
    pair = jnp.concatenate([wq[:, at], wk[:, at]], axis=0)
    wcat[at, : 2 * wq.shape[0]] = jnp.transpose(pair.astype(F32)).astype(BF16)


def pack_rows(plan, lens_ref, tokens, x, trow, bounds, send):
    lens = jnp.broadcast_to(lens_ref[...].astype(F32), (8, plan.batch)).astype(BF16)
    wide = (plan.batch, plan.slots)
    sequence = lax.broadcasted_iota(jnp.int32, wide, 0)
    owner = lax.div(lax.broadcasted_iota(jnp.int32, wide, 1), plan.block_len)
    before = jnp.where(sequence < owner, 1.0, 0.0).astype(BF16)
    same = jnp.where(sequence == owner, 1.0, 0.0).astype(BF16)
    start = jnp.dot(lens, before, preferred_element_type=F32)
    count = jnp.dot(lens, same, preferred_element_type=F32)
    slot = lax.rem(lax.broadcasted_iota(jnp.int32, start.shape, 1), plan.block_len).astype(F32)
    trow[...] = jnp.where(slot < count, start + slot, -1.0)
    square = (plan.batch, plan.batch)
    earlier = lax.broadcasted_iota(jnp.int32, square, 0) < lax.broadcasted_iota(jnp.int32, square, 1)
    begin = jnp.dot(lens, jnp.where(earlier, 1.0, 0.0).astype(BF16), preferred_element_type=F32)
    bounds[0:8, :] = begin
    bounds[8:16, :] = begin + lens.astype(F32)
    base = lax.broadcasted_iota(jnp.int32, (plan.size, plan.slots), 0).astype(F32)
    for j in range(plan.pieces):
        hot = jnp.where(base + float(j * plan.size) == trow[0:1, :], 1.0, 0.0).astype(BF16)
        x[plan.piece(j), :] = jnp.dot(hot, tokens[...], preferred_element_type=F32).astype(BF16)
        send(j)


def row_unit(plan, bounds, rope, tcol, bcol, table, u):
    at = pl.ds(pl.multiple_of(u * plan.size, plan.size), plan.size)
    shape = (plan.size, plan.batch)
    row = (lax.broadcasted_iota(jnp.int32, shape, 0) + u * plan.size).astype(F32)
    begin, end = bounds[0:1, :], bounds[8:9, :]
    inside = (row >= begin) & (row < end)
    slot = jnp.sum(jnp.where(inside, row - begin, 0.0), axis=-1, keepdims=True)
    owner = jnp.sum(jnp.where(row >= end, 1.0, 0.0), axis=-1, keepdims=True)
    full = (plan.size, 128)
    slot = jnp.broadcast_to(slot, full)
    tcol[at, :] = slot
    bcol[at, :] = jnp.broadcast_to(owner, full).astype(BF16)
    lane = lax.broadcasted_iota(jnp.int32, full, 1)
    pick = (lax.rem(lane, plan.block_len).astype(F32) == slot) & (lane < 3 * plan.block_len)
    pick = jnp.where(pick, 1.0, 0.0).astype(BF16)
    table[at, :] = jnp.dot(pick, rope[...], preferred_element_type=F32)


def slot_unit(plan, rate, lens_ref, tgt, onward, hot, u):
    at = pl.ds(pl.multiple_of(u * plan.unit, plan.unit), plan.unit)
    lens = jnp.broadcast_to(lens_ref[...].astype(F32), (plan.unit, plan.batch)).astype(BF16)
    shape = (plan.unit, plan.batch)
    owner = lax.div(lax.broadcasted_iota(jnp.int32, shape, 0), plan.block_len) + u * plan.group
    sequence = lax.broadcasted_iota(jnp.int32, shape, 1)
    before = jnp.where(sequence < owner, 1.0, 0.0).astype(BF16)
    same = jnp.where(sequence == owner, 1.0, 0.0).astype(BF16)
    dims = (((1,), (1,)), ((), ()))
    start = lax.dot_general(before, lens, dims, preferred_element_type=F32)
    count = lax.dot_general(same, lens, dims, preferred_element_type=F32)
    full = (plan.unit, plan.unit)
    slot = lax.rem(lax.broadcasted_iota(jnp.int32, full, 0), plan.block_len).astype(F32)
    target = jnp.where(slot < count, start + slot, -1.0)
    tgt[at, :] = target
    onward[at, :] = jnp.exp(rate * jnp.maximum(count - 1.0 - slot, 0.0))
    moved = jnp.where(target >= 0.0, target + float(FRONT), -1.0)
    lane = lax.broadcasted_iota(jnp.int32, full, 1).astype(F32)
    for c in range(plan.long // 128):
        hot[at, c * 128 : (c + 1) * 128] = jnp.where(moved == lane + float(c * 128), 1.0, 0.0).astype(BF16)


def split_unit(plan, state, halves, u):
    at = pl.ds(pl.multiple_of(u * plan.group, plan.group), plan.group)
    rows = plan.group * plan.key_dim
    whole = state[at].reshape(rows, plan.value_dim)
    high = whole.astype(BF16)
    to = pl.ds(pl.multiple_of(u * rows, rows), rows)
    halves[to, : plan.value_dim] = high
    halves[to, plan.value_dim :] = (whole - high.astype(F32)).astype(BF16)


def state_unit(plan, lens_smem, powers, me, hot, kv, onward, state, u):
    at = pl.ds(pl.multiple_of(u * plan.unit, plan.unit), plan.unit)
    both = 2 * plan.key_dim
    padded = jnp.dot(hot[at, :], kv[...], preferred_element_type=F32)
    values = padded[:, both:].astype(BF16)
    scaled = padded[:, :both] * onward[at, :]
    high = scaled.astype(BF16).astype(F32)
    stacked = jnp.concatenate([high, scaled - high], axis=0)
    wide = (2 * plan.unit, plan.group * plan.key_dim)
    own = lax.rem(
        lax.div(lax.broadcasted_iota(jnp.int32, wide, 0), plan.block_len), plan.group
    ) == lax.div(lax.broadcasted_iota(jnp.int32, wide, 1), plan.key_dim)
    spread = jnp.where(own, jnp.concatenate([stacked] * (plan.group // 2), axis=1), 0.0)
    added = lax.dot_general(
        spread.astype(BF16),
        jnp.concatenate([values, values], axis=0),
        (((0,), (0,)), ((), ())),
        preferred_element_type=F32,
    )
    for b in range(plan.group):
        which = u * plan.group + b
        decay = powers[me, lens_smem[which]]
        state[which] = state[which] * decay + added[b * plan.key_dim : (b + 1) * plan.key_dim, :]


def retention_block(plan, rate, block, queries, kv, gate, tcol, bcol, fade, halves):
    both = 2 * plan.key_dim
    inner = []
    shape = (plan.size, 128)
    gap = lax.broadcasted_iota(jnp.int32, shape, 0) - lax.broadcasted_iota(jnp.int32, shape, 1)
    gap = (gap + FRONT).astype(F32)
    for j in range(*block):
        window = pl.ds(j * plan.size, 128)
        scores = lax.dot_general(
            queries[plan.piece(j), :],
            kv[window, :both],
            (((1,), (1,)), ((), ())),
            preferred_element_type=F32,
        )
        weights = jnp.where(gap <= tcol[plan.piece(j), :], scores * fade[...], 0.0).astype(BF16)
        inner.append(jnp.dot(weights, kv[window, both:], preferred_element_type=F32))
    at = plan.span(block)
    low = plan.first_sequence(block[0] * plan.size) // 2
    high = plan.last_sequence(block[1] * plan.size - 1) // 2 + 1
    q, owner = queries[at, :], bcol[at, :]
    lane = lax.broadcasted_iota(jnp.int32, (q.shape[0], both), 1)
    pick = owner - jnp.where(lane < plan.key_dim, 0.0, 1.0).astype(BF16)
    zero = jnp.zeros_like(q)
    spread = [jnp.where(pick == jnp.asarray(2.0 * c, BF16), q, zero) for c in range(low, high)]
    middle = (low + high) // 2
    carried = None
    for first, last in ((low, middle), (middle, high)):
        term = jnp.dot(
            jnp.concatenate(spread[first - low : last - low], axis=1),
            halves[first * both : last * both, :],
            preferred_element_type=F32,
        )
        carried = term if carried is None else carried + term
    carried = carried[:, : plan.value_dim] + carried[:, plan.value_dim :]
    retained = jnp.concatenate(inner, axis=0) + carried * jnp.exp(rate * (tcol[at, :] + 1.0))
    inv = lax.rsqrt(jnp.mean(retained * retained, axis=-1, keepdims=True) + NORM_EPSILON)
    return (retained * inv * gate[at, :]).astype(BF16)


class Scatter:
    def __init__(self, ring, h_pair, w_pair, outbox, inbox, parts, sems):
        self.ring, self.plan = ring, ring.plan
        self.h_pair, self.w_pair, self.outbox, self.inbox, self.parts = h_pair, w_pair, outbox, inbox, parts
        self.out, self.recv, self.pair_recv = sems

    def offer(self, k):
        rows, depth = self.plan.span(self.plan.blocks[k]), self.plan.value_dim
        return remote(
            self.h_pair.at[rows, pl.ds(0, depth)],
            self.h_pair.at[rows, pl.ds(depth, depth)],
            self.out.at[1],
            self.pair_recv.at[k],
            self.ring.partner,
        )

    def hop(self, j, way, i):
        return remote(
            self.outbox.at[j, way, i - 1],
            self.inbox.at[j, way, i - 1],
            self.out.at[0],
            self.recv.at[j, way, i - 1],
            self.ring.next[way],
        )

    def prepare(self, k, distance):
        plan = self.plan
        ways = (0, 1) if 0 < distance < plan.far else (0,)
        at = plan.span(plan.blocks[k])
        columns = []
        for way in ways:
            target = self.ring.ahead(way, distance)
            columns.append(self.w_pair[:, pl.ds(pl.multiple_of(target * plan.width, plan.width), plan.width)])
        part = jnp.dot(
            self.h_pair[at, :], jnp.concatenate(columns, axis=1), preferred_element_type=F32
        )
        for way in ways:
            self.parts[way, distance % 2, at, :] = part[:, way * plan.width : (way + 1) * plan.width]

    def begin(self, k):
        plan = self.plan
        self.offer(k).wait_recv()
        self.prepare(k, plan.far)
        for j in range(*plan.blocks[k]):
            way = j % 2
            self.outbox[j, way, 0] = self.parts[0, plan.far % 2, plan.piece(j), :].astype(BF16)
            self.hop(j, way, 1).start()
        self.prepare(k, plan.far - 1)
        for j in range(*plan.blocks[k]):
            way = 1 - j % 2
            self.outbox[j, way, 0] = self.parts[way, (plan.far - 1) % 2, plan.piece(j), :].astype(BF16)
            self.hop(j, way, 1).start()
        self.prepare(k, plan.far - 2)

    def arrive(self, j, way, i):
        distance = self.plan.reach(j, way) - i
        if distance <= 0:
            return
        self.hop(j, way, i).wait_recv()
        part = self.parts[way, distance % 2, self.plan.piece(j), :] + self.inbox[j, way, i - 1].astype(F32)
        self.outbox[j, way, i] = part.astype(BF16)
        self.hop(j, way, i + 1).start()

    def round(self, k, i):
        plan = self.plan
        for j in range(*plan.blocks[k]):
            for way in (0, 1):
                self.arrive(j, way, i)
        if plan.far - 2 - i >= 0:
            self.prepare(k, plan.far - 2 - i)

    def last(self, j):
        plan = self.plan
        total = self.parts[0, 0, plan.piece(j), :]
        for way in (1 - j % 2, j % 2):
            reach = plan.reach(j, way)
            self.hop(j, way, reach).wait_recv()
            total = total + self.inbox[j, way, reach - 1].astype(F32)
        return total.astype(BF16).astype(F32)

    def drain(self, whole):
        every = whole.at[:, pl.ds(0, (self.plan.m - 1) * self.plan.width)]
        remote(every, every, self.out.at[0], self.pair_recv.at[0], self.ring.partner).wait_send()
        half = self.h_pair.at[:, pl.ds(0, self.plan.value_dim)]
        remote(half, half, self.out.at[1], self.pair_recv.at[0], self.ring.partner).wait_send()


def whole_kernel(plan, *refs):
    (lens_smem, powers, rates, lens_ref, tokens, rope, *rest) = refs
    gains, raw, outs_w, states_in, (mixed, *states), scratch = (
        (rest[0], rest[7]),
        (rest[1:5], rest[8:12]),
        (rest[5], rest[12]),
        (rest[6], rest[13]),
        rest[14:17],
        rest[17:],
    )
    (x, x1, y, whole, wcats, turned, w_pairs, total, squares, table, gate, tcol, bcol, queries) = scratch[:14]
    (kv, halves, hot, onward, tgt, parts, outbox, inbox, h_pair, trow, bounds, fade) = scratch[14:26]
    load, pair_w = scratch[26:28]
    sems = scratch[28:]
    ring = Ring(plan)
    ring.greet()
    depth, both = plan.value_dim, 2 * plan.key_dim
    rate = rates[0, ring.me]

    loads = {}
    for i in range(2):
        wq, wk, wv, wg = raw[i]
        targets = (
            (wq, turned.at[i, 0]),
            (wk, turned.at[i, 1]),
            (wv, wcats.at[i, :, pl.ds(both, depth)]),
            (wg, wcats.at[i, :, pl.ds(both + depth, depth)]),
            (outs_w[i], w_pairs.at[i, pl.ds(0, depth), :]),
            (states_in[i], states[i]),
        )
        for k, (source, target) in enumerate(targets):
            loads[i, k] = pltpu.make_async_copy(source, target, load.at[i, k])

    def swap(i):
        return remote(
            w_pairs.at[i, pl.ds(0, depth), :],
            w_pairs.at[i, pl.ds(depth, depth), :],
            pair_w.at[0, i],
            pair_w.at[1, i],
            ring.partner,
        )

    gathers = [Gather(ring, (x, x1)[i], whole, sems[:3]) for i in range(2)]
    scatters = [
        Scatter(ring, h_pair, w_pairs.at[i], outbox, inbox, parts, sems[3:])
        for i in range(2)
    ]
    projections = [Projection(gathers[i], gains[i], wcats.at[i], total, squares) for i in range(2)]

    for k in range(6):
        loads[0, k].start()
    met = []

    def send(j):
        if not met:
            ring.met()
            met.append(1)
        gathers[0].begin(j)

    pack_rows(plan, lens_ref, tokens, x, trow, bounds, send)
    for k in range(6):
        loads[1, k].start()
    loads[0, 0].wait()
    loads[0, 1].wait()

    @pl.loop(0, wcats.shape[1] // 128)
    def _(u):
        fill_unit(turned.at[0, 0], turned.at[0, 1], wcats.at[0], u)

    loads[0, 2].wait()
    loads[0, 3].wait()
    shape = (plan.size, 128)
    gap = lax.broadcasted_iota(jnp.int32, shape, 0) - lax.broadcasted_iota(jnp.int32, shape, 1)
    gap = (gap + FRONT).astype(F32)
    near = (gap >= 0.0) & (gap < float(plan.block_len))
    fade[...] = jnp.where(near, 0.5 * jnp.exp(rate * jnp.maximum(gap, 0.0)), 0.0)
    kv[:FRONT, :] = jnp.zeros((FRONT, kv.shape[1]), BF16)
    kv[FRONT + plan.rows :, :] = jnp.zeros((plan.long - FRONT - plan.rows, kv.shape[1]), BF16)
    y[:FRONT, :] = jnp.zeros((FRONT, plan.width), BF16)
    y[FRONT + plan.rows :, :] = jnp.zeros((plan.long - FRONT - plan.rows, plan.width), BF16)
    loads[0, 5].wait()
    loads[0, 4].wait()
    swap(0).start()

    def run(i, gather_work, scatter_work, finish):
        gather, projection, scatter = gathers[i], projections[i], scatters[i]
        far, blocks = plan.far, plan.blocks

        def step(k, h):
            for j in range(*blocks[k]):
                for way in (0, 1):
                    gather.arrive(j, way, h)
            projection.add(k, h - 1)
            if gather_work:
                gather_work.pop(0)()

        for h in range(1, far):
            for k in range(len(blocks)):
                step(k, h)

        def project(k):
            projection.finish(blocks[k], table, queries, kv, gate)

        def retain(k):
            h_pair[plan.span(blocks[k]), :depth] = retention_block(
                plan, rate, blocks[k], queries, kv, gate, tcol, bcol, fade, halves
            )
            scatter.offer(k).start()

        def round(k, r):
            scatter.round(k, r)
            if r > 1 and scatter_work:
                scatter_work.pop(0)()

        many = len(blocks)
        ahead = 3
        for k in range(min(ahead, many)):
            step(k, far)
        for k in range(many):
            project(k)
            retain(k)
            if k + ahead < many:
                step(k + ahead, far)
            elif gather_work:
                while gather_work:
                    gather_work.pop(0)()
            if k == 0:
                swap(i).wait_recv()
            else:
                scatter.begin(k - 1)
            if k >= 3:
                round(k - 3, 1)
        gather.drain()
        round(many - 3, 1)
        scatter.begin(many - 1)
        for k in (many - 2, many - 1):
            round(k, 1)
        for r in range(2, far):
            for k in range(many):
                round(k, r)
        while scatter_work:
            scatter_work.pop(0)()
        for j in range(plan.pieces):
            finish(j, scatter.last(j))

    def every(first, last, unit_work):
        def act():
            @pl.loop(first, last)
            def _(u):
                unit_work(u)

        return act

    units = plan.units

    def update(i, times):
        body = lambda u: state_unit(plan, lens_smem, powers, ring.me, hot, kv, onward, states[i], u)
        return spread_out(units, times, body)

    def halve(i):
        return every(0, units, lambda u: split_unit(plan, states[i], halves, u))

    slot_body = lambda u: slot_unit(plan, rate, lens_ref, tgt, onward, hot, u)
    row_body = lambda u: row_unit(plan, bounds, rope, tcol, bcol, table, u)
    spread_out = lambda total, times, body: [
        every(total * k // times, total * (k + 1) // times, body) for k in range(times)
    ]
    first_work = spread_out(plan.pieces, 2, row_body) + [halve(0)] + spread_out(units, 4, slot_body)

    def after_first(j, mix):
        at = plan.piece(j)
        x1[at, :] = (x[at, :].astype(F32) + mix).astype(BF16)
        gathers[1].begin(j)

    def ready_second():
        for k in range(6):
            loads[1, k].wait()
        swap(1).start()

        @pl.loop(0, wcats.shape[1] // 128)
        def _(u):
            fill_unit(turned.at[1, 0], turned.at[1, 1], wcats.at[1], u)

    run(0, first_work, [ready_second], after_first)
    scatters[0].drain(whole)
    swap(0).wait_send()

    def after_second(j, mix):
        at = plan.piece(j)
        y[pl.ds(FRONT + j * plan.size, plan.size), :] = (x1[at, :].astype(F32) + mix).astype(BF16)

    run(1, [halve(1)] + update(0, 6), update(1, 6), after_second)
    scatters[1].drain(whole)
    swap(1).wait_send()
    many = next(k for k in (3, 2, 1) if plan.units % k == 0)

    @pl.loop(0, plan.units // many)
    def _(u):
        at = pl.ds(pl.multiple_of(u * many * plan.unit, plan.unit), many * plan.unit)
        spread = jnp.dot(hot[at, :], y[...], preferred_element_type=F32)
        live = jnp.concatenate([tgt[at, :]] * (plan.width // 128), axis=1) >= 0.0
        mixed[at, :] = jnp.where(live, spread, tokens[at, :].astype(F32)).astype(BF16)


def fused(plan, heads, lengths, tokens, first, second):
    total_heads = heads
    logs = np.log(1.0 - 2.0 ** (-1.5 - 6.0 * np.arange(total_heads) / (total_heads - 1)))
    powers = np.exp(logs[:, None] * np.arange(plan.block_len + 1)[None, :]).astype(np.float32)
    half = plan.key_dim // 2
    inverse = np.float32(ROPE_BASE) ** (-np.arange(half, dtype=np.float32) / np.float32(half))
    positions = PAST_LEN + np.arange(plan.block_len, dtype=np.float32)
    angles = (positions[:, None] * inverse.astype(np.float32)[None, :]).astype(np.float64)
    cosines, sines = np.cos(angles), np.sin(angles)
    cosines = np.concatenate([cosines, cosines], axis=1)
    sines = np.concatenate([-sines, sines], axis=1)
    scale = plan.key_dim**-0.5
    rope = np.concatenate([cosines, cosines * scale, sines, sines * scale], axis=1).astype(np.float32)
    stacked, rest = [], rope
    for _ in range(3):
        stacked.append(rest.astype(jnp.bfloat16))
        rest = rest - stacked[-1].astype(np.float32)
    rope = np.zeros((128, rope.shape[1]), jnp.bfloat16)
    rope[: 3 * plan.block_len] = np.concatenate(stacked, axis=0)

    n, rows, width = plan.n, plan.rows, plan.width
    wide, both = 2 * plan.key_dim + 2 * plan.value_dim, 2 * plan.key_dim
    depth = plan.value_dim
    model = n * width
    state_shape = (plan.batch, plan.key_dim, plan.value_dim)
    vmem = lambda shape, kind: pltpu.VMEM(shape, kind)
    dma = lambda *shape: pltpu.SemaphoreType.DMA(shape)
    scratch = [
        vmem((rows, width), BF16),
        vmem((rows, width), BF16),
        vmem((plan.long, width), BF16),
        vmem((rows, model), BF16),
        vmem((2, model, wide), BF16),
        vmem((2, 2, plan.key_dim, model), BF16),
        vmem((2, 2 * depth, model), BF16),
        vmem((rows, wide), F32),
        vmem((rows, 128), F32),
        vmem((rows, 2 * both), F32),
        vmem((rows, depth), F32),
        vmem((rows, 128), F32),
        vmem((rows, 128), BF16),
        vmem((rows, both), BF16),
        vmem((plan.long, both + depth), BF16),
        vmem((plan.batch * plan.key_dim, 2 * depth), BF16),
        vmem((plan.slots, plan.long), BF16),
        vmem((plan.slots, 128), F32),
        vmem((plan.slots, 128), F32),
        vmem((2, 2, rows, width), F32),
        vmem((plan.pieces, 2, plan.far, plan.size, width), BF16),
        vmem((plan.pieces, 2, plan.far, plan.size, width), BF16),
        vmem((rows, 2 * depth), BF16),
        vmem((8, plan.slots), F32),
        vmem((16, plan.batch), F32),
        vmem((plan.size, 128), F32),
        dma(2, 6),
        dma(2, 2),
    ]
    scratch += [dma(2), dma(plan.pieces, 2, plan.far), dma(len(plan.blocks), plan.far + 1)]
    scratch += [dma(2), dma(plan.pieces, 2, plan.far), dma(len(plan.blocks))]
    spec = lambda space: pl.BlockSpec(memory_space=space)
    inside, outside, scalars = spec(pltpu.VMEM), spec(pltpu.HBM), spec(pltpu.SMEM)

    def group(gain, query, key, value, gate, out, state):
        far = [
            pltpu.with_memory_space_constraint(a, pltpu.HBM)
            for a in (query.T, key.T, value, gate, out, state.reshape(state_shape))
        ]
        return (gain[None], *far)

    block_specs = [inside] + [outside] * 6

    mixed, one, two = pl.pallas_call(
        functools.partial(whole_kernel, plan),
        out_shape=[
            pltpu.VMEM((plan.slots, width), BF16),
            pltpu.VMEM(state_shape, F32),
            pltpu.VMEM(state_shape, F32),
        ],
        in_specs=[scalars] * 3 + [inside] * 3 + block_specs * 2,
        out_specs=[inside, inside, inside],
        scratch_shapes=scratch,
        compiler_params=pltpu.CompilerParams(
            collective_id=0, has_side_effects=True, vmem_limit_bytes=48 * 2**20
        ),
    )(
        lengths,
        jnp.asarray(powers),
        jnp.asarray(logs.astype(np.float32)[None, :]),
        lengths[None, :],
        tokens,
        jnp.asarray(rope),
        *group(*first),
        *group(*second),
    )
    return mixed, one.reshape(first[-1].shape), two.reshape(second[-1].shape)


def unpacked(lengths, tokens, first, second):
    batch_size, head_count, key_dim, value_dim = first[-1].shape
    slots = tokens.shape[0]
    block_len = slots // batch_size
    table = jnp.tile(rope_tables(block_len, key_dim), (batch_size, 1))
    x, states = tokens, []
    for gain, query, key, value, gate, out, state in (first, second):
        qk = []
        for weight in (query, key):
            qk.append(weight.reshape(weight.shape[0], head_count, key_dim))
        x, new_state = plain_block(x, lengths, gain, qk, value, gate, out, state, table)
        states.append(new_state)
    return (x, *states)


def shards(
    tokens,
    lengths,
    gain_first,
    query_first,
    key_first,
    value_first,
    gate_first,
    out_first,
    state_first,
    gain_second,
    query_second,
    key_second,
    value_second,
    gate_second,
    out_second,
    state_second,
):
    n = lax.axis_size("tp")
    batch_size, head_count, key_dim, value_dim = state_first.shape
    slots, width = tokens.shape
    block_len = slots // batch_size
    rows = LIVE_TOTAL
    lengths = lengths.astype(jnp.int32)
    first = (gain_first, query_first, key_first, value_first, gate_first, out_first, state_first)
    second = (gain_second, query_second, key_second, value_second, gate_second, out_second, state_second)
    pieces = next((p for p in (10, 8, 6, 4) if rows % (16 * p) == 0 and rows // p <= 128 - FRONT), 0)
    fits = (
        n >= 12
        and n % 4 == 0
        and pieces >= 8
        and head_count == 1
        and width == 128
        and value_dim == 128
        and key_dim == 64
        and block_len <= FRONT
        and 128 % (2 * block_len) == 0
        and 3 * block_len <= 128
        and batch_size <= 128
        and batch_size % 2 == 0
        and slots % 128 == 0
    )
    if not fits:
        return unpacked(lengths, tokens, first, second)
    plan = Plan(n, rows, pieces, batch_size, block_len, key_dim, value_dim, width)
    return fused(plan, n * head_count, lengths, tokens, first, second)


def solution(mesh):
    heads = P(None, "tp")
    state = P("grp", "tp", None, None)
    block = (P(), heads, heads, heads, heads, P("tp", None), state)
    in_specs = (P("grp", "tp"), P("grp")) + block + block
    out_specs = (P("grp", "tp"), state, state)
    return jax.shard_map(shards, mesh=mesh, in_specs=in_specs, out_specs=out_specs, check_vma=False)
```

```python
import functools

import jax
import jax.numpy as jnp
from jax import lax
from jax.experimental import pallas as pl
from jax.experimental.pallas import tpu as pltpu
from jax.sharding import PartitionSpec as P
import numpy as np

PAST_LEN = 16384
LIVE_TOTAL = 960

NORM_EPSILON = 1e-06
ROPE_BASE = 10000.0

MESH = pl.DeviceIdType.MESH
F32 = jnp.float32
BF16 = jnp.bfloat16


def decay_logs(head_count):
    head_total = lax.axis_size("tp") * head_count
    head_ids = (lax.axis_index("tp") * head_count + jnp.arange(head_count)).astype(F32)
    return jnp.log(1.0 - 2.0 ** (-1.5 - 6.0 * head_ids / (head_total - 1)))


def rope_tables(block_len, key_dim):
    half_dim = key_dim // 2
    inverse = ROPE_BASE ** (-jnp.arange(half_dim, dtype=F32) / half_dim)
    positions = PAST_LEN + jnp.arange(block_len, dtype=F32)
    angles = positions[:, None] * inverse[None, :]
    cosines, sines = jnp.cos(angles), jnp.sin(angles)
    cosines = jnp.concatenate([cosines, cosines], axis=1)
    sines = jnp.concatenate([-sines, sines], axis=1)
    scale = key_dim ** (-0.5)
    return jnp.concatenate([cosines, cosines * scale, sines, sines * scale], axis=1)


def retain(queries, key_rows, values, lengths, state_in):
    batch_size, head_count, key_dim, value_dim = state_in.shape
    block_len = queries.shape[0] // batch_size
    log_gamma = decay_logs(head_count)
    queries = queries.reshape(batch_size, block_len, head_count, key_dim)
    key_rows = key_rows.reshape(batch_size, block_len, head_count, key_dim)
    values = values.reshape(batch_size, block_len, head_count, value_dim)
    slot_ids = jnp.arange(block_len).astype(F32)
    live_count = lengths.astype(F32)
    active = (slot_ids[None, :] < live_count[:, None]).astype(F32)
    step_gap = slot_ids[:, None] - slot_ids[None, :]
    causal = (step_gap >= 0.0).astype(F32)
    within = jnp.exp(log_gamma[:, None, None] * jnp.maximum(step_gap, 0.0)[None]) * causal[None]
    scores = jnp.einsum("bihd,bjhd->bhij", queries, key_rows, preferred_element_type=F32)
    weights = (scores * within[None]).astype(BF16)
    inner_part = jnp.einsum("bhij,bjhe->bihe", weights, values, preferred_element_type=F32)
    carried = jnp.einsum(
        "bihd,bhde->bihe", queries.astype(F32), state_in, precision=lax.Precision.HIGHEST
    )
    carried = (
        carried * jnp.exp(log_gamma[None, None, :] * (slot_ids[None, :, None] + 1.0))[..., None]
    )
    retained = (inner_part + carried) * active[:, :, None, None]
    lead_gap = live_count[:, None] - 1.0 - slot_ids[None, :]
    key_weight = (
        jnp.exp(log_gamma[None, None, :] * jnp.maximum(lead_gap, 0.0)[:, :, None])
        * active[:, :, None]
    )
    added_state = jnp.einsum(
        "bjhd,bjhe->bhde",
        key_rows.astype(F32) * key_weight[..., None],
        values.astype(F32),
        precision=lax.Precision.HIGHEST,
    )
    new_state = (
        state_in * jnp.exp(log_gamma[None, :] * live_count[:, None])[:, :, None, None] + added_state
    )
    inv_rms = lax.rsqrt(jnp.mean(retained * retained, axis=-1, keepdims=True) + NORM_EPSILON)
    return (retained * inv_rms).reshape(batch_size * block_len, -1), new_state


def rotated(vectors, table, scale_at):
    key_dim = vectors.shape[-1]
    half = key_dim // 2
    swapped = jnp.concatenate([vectors[..., half:], vectors[..., :half]], axis=-1)
    cosines = table[:, None, scale_at * key_dim : (scale_at + 1) * key_dim]
    sines = table[:, None, (2 + scale_at) * key_dim : (3 + scale_at) * key_dim]
    return (vectors * cosines + swapped * sines).astype(BF16)


def plain_block(x, lengths, gain, qk_weights, w_value, w_gate, w_out, state, table):
    batch_size, head_count, key_dim, value_dim = state.shape
    whole = lax.all_gather(x, "tp", axis=1, tiled=True).astype(F32)
    inv = lax.rsqrt(jnp.mean(whole * whole, axis=-1, keepdims=True) + NORM_EPSILON)
    normed = (whole * inv * gain).astype(BF16)
    turned = []
    for scale_at, weight in enumerate(qk_weights):
        product = jnp.einsum("rd,dhk->rhk", normed, weight, preferred_element_type=F32)
        turned.append(rotated(product, table, scale_at))
    values = jnp.dot(normed, w_value, preferred_element_type=F32).astype(BF16)
    gate = jnp.dot(normed, w_gate, preferred_element_type=F32)
    retained, new_state = retain(turned[0], turned[1], values, lengths, state)
    heads_out = (retained * jax.nn.silu(gate)).astype(BF16)
    part = jnp.dot(heads_out, w_out, preferred_element_type=F32).astype(BF16)
    mix = lax.psum_scatter(part, "tp", scatter_dimension=1, tiled=True)
    return (x.astype(F32) + mix.astype(F32)).astype(BF16), new_state


FRONT = 32


class Plan:
    def __init__(self, n, rows, pieces, batch, block_len, key_dim, value_dim, width):
        self.n, self.m, self.far = n, n // 2, n // 4
        self.rows, self.pieces, self.size = rows, pieces, rows // pieces
        self.batch, self.block_len = batch, block_len
        self.key_dim, self.value_dim, self.width = key_dim, value_dim, width
        self.slots = batch * block_len
        self.unit = 128
        self.units = self.slots // self.unit
        self.group = self.unit // block_len
        self.long = -(-(rows + FRONT) // 128) * 128
        self.blocks = [(j, j + 2) for j in range(0, pieces, 2)]
        lead = -(-3 * len(self.blocks) // 5)
        self.leading = list(range(lead))
        self.trailing = list(range(lead, len(self.blocks)))

    def reach(self, j, way):
        return self.far if j % 2 == way else self.far - 1

    def piece(self, j):
        return pl.ds(j * self.size, self.size)

    def span(self, block):
        return pl.ds(block[0] * self.size, (block[1] - block[0]) * self.size)

    def first_sequence(self, row):
        return max(row // self.block_len, self.batch - self.rows + row)

    def last_sequence(self, row):
        return min(row, self.batch - -(-(self.rows - row) // self.block_len))


class Ring:
    def __init__(self, plan):
        self.plan, self.m = plan, plan.m
        me = lax.axis_index("tp")
        self.core = lax.rem(me, 2)
        chip = lax.div(me, 2)
        odd = lax.rem(chip, 2)
        half = lax.div(chip, 2)
        self.pos = (1 - odd) * half + odd * (self.m - 1 - half)
        self.me = me
        self.partner = chip * 2 + 1 - self.core
        self.next = (self.device(self.pos + 1), self.device(self.pos - 1))

    def device(self, pos):
        m = self.m
        pos = lax.rem(pos + m, m)
        far = lax.div(pos, m // 2)
        chip = (1 - far) * 2 * pos + far * (2 * (m - 1 - pos) + 1)
        return chip * 2 + self.core

    def greet(self):
        barrier = pltpu.get_barrier_semaphore()
        for device in (*self.next, self.partner):
            pl.semaphore_signal(barrier, inc=1, device_id={"tp": device}, device_id_type=MESH)

    def met(self):
        pl.semaphore_wait(pltpu.get_barrier_semaphore(), 3)

    def behind(self, way, steps):
        return self.device(self.pos - steps if way == 0 else self.pos + steps)

    def ahead(self, way, steps):
        return self.device(self.pos + steps if way == 0 else self.pos - steps)


def remote(src, dst, send, recv, device):
    return pltpu.make_async_remote_copy(
        src_ref=src,
        dst_ref=dst,
        send_sem=send,
        recv_sem=recv,
        device_id={"tp": device},
        device_id_type=MESH,
    )


class Gather:
    def __init__(self, ring, own, whole, sems):
        self.ring, self.plan, self.own, self.whole = ring, ring.plan, own, whole
        self.out, self.recv, self.share_recv = sems

    def columns(self, device):
        return pl.ds(pl.multiple_of(device * self.plan.width, self.plan.width), self.plan.width)

    def place(self, j, way, h):
        return self.whole.at[self.plan.piece(j), self.columns(self.ring.behind(way, h))]

    def source(self, j, way, h):
        return self.own.at[self.plan.piece(j), :] if h == 0 else self.place(j, way, h)

    def hop(self, j, way, h):
        return remote(
            self.source(j, way, h - 1),
            self.place(j, way, h - 1),
            self.out.at[0],
            self.recv.at[j, way, h - 1],
            self.ring.next[way],
        )

    def share(self, j, way, h):
        return remote(
            self.source(j, way, h),
            self.place(j, way, h),
            self.out.at[1],
            self.share_recv.at[j // 2, h],
            self.ring.partner,
        )

    def begin(self, j):
        for way in (0, 1):
            self.hop(j, way, 1).start()
        self.share(j, 0, 0).start()
        self.whole[self.plan.piece(j), self.columns(self.ring.me)] = self.own[self.plan.piece(j), :]

    def arrive(self, j, way, h):
        reach = self.plan.reach(j, way)
        if h > reach:
            return
        self.hop(j, way, h).wait_recv()
        if h < reach:
            self.hop(j, way, h + 1).start()
        self.share(j, way, h).start()

    def shared(self, k, h):
        wide = self.plan.width if h in (0, self.plan.far) else 2 * self.plan.width
        every = self.whole.at[self.plan.span(self.plan.blocks[k]), pl.ds(0, wide)]
        remote(every, every, self.out.at[1], self.share_recv.at[k, h], self.ring.partner).wait_recv()

    def drain(self):
        for k, count in enumerate((self.plan.m - 1, self.plan.m)):
            every = self.whole.at[:, pl.ds(0, count * self.plan.width)]
            remote(every, every, self.out.at[k], self.share_recv.at[0, 0], self.ring.partner).wait_send()


class Projection:
    def __init__(self, gather, gain, wcat, total, squares):
        self.gather, self.plan, self.ring = gather, gather.plan, gather.ring
        self.gain, self.wcat, self.total, self.squares = gain, wcat, total, squares

    def product(self, at, h):
        plan = self.plan
        product, part = None, None
        for way in (0, 1) if 0 < h < plan.far else (0,):
            chip = lax.div(self.ring.behind(way, h), 2)
            cols = pl.ds(pl.multiple_of(chip * 2 * plan.width, 2 * plan.width), 2 * plan.width)
            x = self.gather.whole[at, cols].astype(F32)
            square = x * x
            for k in range(0, 2 * plan.width, 128):
                part = square[:, k : k + 128] if part is None else part + square[:, k : k + 128]
            scaled = (x * self.gain[:, cols]).astype(BF16)
            term = jnp.dot(scaled, self.wcat[cols, :], preferred_element_type=F32)
            product = term if product is None else product + term
        return product, part

    def add(self, k, h):
        plan = self.plan
        block = plan.blocks[k]
        self.gather.shared(k, h)
        at = plan.span(block)
        product, part = self.product(at, h)
        if h == 0:
            self.total[at, :], self.squares[at, :] = product, part
        else:
            self.total[at, :] += product
            self.squares[at, :] += part

    def finish(self, block, table, queries, kv, gate):
        plan = self.plan
        at = plan.span(block)
        self.gather.shared(plan.blocks.index(block), plan.far)
        product, part = self.product(at, plan.far)
        square = self.squares[at, :] + part
        mean = jnp.sum(square, axis=-1, keepdims=True) / (plan.n * plan.width)
        out = (self.total[at, :] + product) * lax.rsqrt(mean + NORM_EPSILON)
        key_dim, both = plan.key_dim, 2 * plan.key_dim
        qk = out[:, :both]
        lane = lax.broadcasted_iota(jnp.int32, qk.shape, 1)
        ahead = pltpu.roll(qk, both - key_dim // 2, 1)
        behind = pltpu.roll(qk, key_dim // 2, 1)
        swapped = jnp.where(lax.rem(lane, key_dim) < key_dim // 2, ahead, behind)
        turned = qk * table[at, :both] + swapped * table[at, both:]
        crossed = pltpu.roll(turned, key_dim, 1)
        front = lane < key_dim
        queries[at, :] = jnp.where(front, turned, crossed).astype(BF16)
        low = pl.ds(FRONT + block[0] * plan.size, (block[1] - block[0]) * plan.size)
        kv[low, :both] = jnp.where(front, crossed, turned).astype(BF16)
        kv[low, both:] = out[:, both : both + plan.value_dim].astype(BF16)
        open_gate = out[:, both + plan.value_dim :]
        gate[at, :] = open_gate / (1.0 + jnp.exp(-open_gate))


def fill_unit(wq, wk, wcat, u):
    at = pl.ds(pl.multiple_of(u * 128, 128), 128)
    pair = jnp.concatenate([wq[:, at], wk[:, at]], axis=0)
    wcat[at, : 2 * wq.shape[0]] = jnp.transpose(pair.astype(F32)).astype(BF16)


def pack_rows(plan, lens_ref, tokens, x, trow, bounds, send):
    lens = jnp.broadcast_to(lens_ref[...].astype(F32), (8, plan.batch)).astype(BF16)
    wide = (plan.batch, plan.slots)
    sequence = lax.broadcasted_iota(jnp.int32, wide, 0)
    owner = lax.div(lax.broadcasted_iota(jnp.int32, wide, 1), plan.block_len)
    before = jnp.where(sequence < owner, 1.0, 0.0).astype(BF16)
    same = jnp.where(sequence == owner, 1.0, 0.0).astype(BF16)
    start = jnp.dot(lens, before, preferred_element_type=F32)
    count = jnp.dot(lens, same, preferred_element_type=F32)
    slot = lax.rem(lax.broadcasted_iota(jnp.int32, start.shape, 1), plan.block_len).astype(F32)
    trow[...] = jnp.where(slot < count, start + slot, -1.0)
    square = (plan.batch, plan.batch)
    earlier = lax.broadcasted_iota(jnp.int32, square, 0) < lax.broadcasted_iota(jnp.int32, square, 1)
    begin = jnp.dot(lens, jnp.where(earlier, 1.0, 0.0).astype(BF16), preferred_element_type=F32)
    bounds[0:8, :] = begin
    bounds[8:16, :] = begin + lens.astype(F32)
    base = lax.broadcasted_iota(jnp.int32, (plan.size, plan.slots), 0).astype(F32)
    for j in range(plan.pieces):
        hot = jnp.where(base + float(j * plan.size) == trow[0:1, :], 1.0, 0.0).astype(BF16)
        x[plan.piece(j), :] = jnp.dot(hot, tokens[...], preferred_element_type=F32).astype(BF16)
        if j // 2 in plan.leading:
            send(j)


def row_unit(plan, bounds, rope, tcol, bcol, table, u):
    at = pl.ds(pl.multiple_of(u * plan.size, plan.size), plan.size)
    shape = (plan.size, plan.batch)
    row = (lax.broadcasted_iota(jnp.int32, shape, 0) + u * plan.size).astype(F32)
    begin, end = bounds[0:1, :], bounds[8:9, :]
    inside = (row >= begin) & (row < end)
    slot = jnp.sum(jnp.where(inside, row - begin, 0.0), axis=-1, keepdims=True)
    owner = jnp.sum(jnp.where(row >= end, 1.0, 0.0), axis=-1, keepdims=True)
    full = (plan.size, 128)
    slot = jnp.broadcast_to(slot, full)
    tcol[at, :] = slot
    bcol[at, :] = jnp.broadcast_to(owner, full).astype(BF16)
    lane = lax.broadcasted_iota(jnp.int32, full, 1)
    pick = (lax.rem(lane, plan.block_len).astype(F32) == slot) & (lane < 3 * plan.block_len)
    pick = jnp.where(pick, 1.0, 0.0).astype(BF16)
    table[at, :] = jnp.dot(pick, rope[...], preferred_element_type=F32)


def slot_unit(plan, rate, lens_ref, tgt, onward, hot, u):
    at = pl.ds(pl.multiple_of(u * plan.unit, plan.unit), plan.unit)
    lens = jnp.broadcast_to(lens_ref[...].astype(F32), (plan.unit, plan.batch)).astype(BF16)
    shape = (plan.unit, plan.batch)
    owner = lax.div(lax.broadcasted_iota(jnp.int32, shape, 0), plan.block_len) + u * plan.group
    sequence = lax.broadcasted_iota(jnp.int32, shape, 1)
    before = jnp.where(sequence < owner, 1.0, 0.0).astype(BF16)
    same = jnp.where(sequence == owner, 1.0, 0.0).astype(BF16)
    dims = (((1,), (1,)), ((), ()))
    start = lax.dot_general(before, lens, dims, preferred_element_type=F32)
    count = lax.dot_general(same, lens, dims, preferred_element_type=F32)
    full = (plan.unit, plan.unit)
    slot = lax.rem(lax.broadcasted_iota(jnp.int32, full, 0), plan.block_len).astype(F32)
    target = jnp.where(slot < count, start + slot, -1.0)
    tgt[at, :] = target
    onward[at, :] = jnp.exp(rate * jnp.maximum(count - 1.0 - slot, 0.0))
    moved = jnp.where(target >= 0.0, target + float(FRONT), -1.0)
    lane = lax.broadcasted_iota(jnp.int32, full, 1).astype(F32)
    for c in range(plan.long // 128):
        hot[at, c * 128 : (c + 1) * 128] = jnp.where(moved == lane + float(c * 128), 1.0, 0.0).astype(BF16)


def split_unit(plan, state, halves, u):
    at = pl.ds(pl.multiple_of(u * plan.group, plan.group), plan.group)
    rows = plan.group * plan.key_dim
    whole = state[at].reshape(rows, plan.value_dim)
    halves[pl.ds(pl.multiple_of(u * rows, rows), rows), :] = whole.astype(BF16)


def state_unit(plan, lens_smem, powers, me, hot, kv, onward, state, u):
    at = pl.ds(pl.multiple_of(u * plan.unit, plan.unit), plan.unit)
    both = 2 * plan.key_dim
    padded = jnp.dot(hot[at, :], kv[...], preferred_element_type=F32)
    values = padded[:, both:].astype(BF16)
    scaled = padded[:, :both] * onward[at, :]
    high = scaled.astype(BF16).astype(F32)
    stacked = jnp.concatenate([high, scaled - high], axis=0)
    wide = (2 * plan.unit, plan.group * plan.key_dim)
    own = lax.rem(
        lax.div(lax.broadcasted_iota(jnp.int32, wide, 0), plan.block_len), plan.group
    ) == lax.div(lax.broadcasted_iota(jnp.int32, wide, 1), plan.key_dim)
    spread = jnp.where(own, jnp.concatenate([stacked] * (plan.group // 2), axis=1), 0.0)
    added = lax.dot_general(
        spread.astype(BF16),
        jnp.concatenate([values, values], axis=0),
        (((0,), (0,)), ((), ())),
        preferred_element_type=F32,
    )
    for b in range(plan.group):
        which = u * plan.group + b
        decay = powers[me, lens_smem[which]]
        state[which] = state[which] * decay + added[b * plan.key_dim : (b + 1) * plan.key_dim, :]


def retention_block(plan, rate, block, queries, kv, gate, tcol, bcol, fade, halves):
    both = 2 * plan.key_dim
    inner = []
    shape = (plan.size, 128)
    gap = lax.broadcasted_iota(jnp.int32, shape, 0) - lax.broadcasted_iota(jnp.int32, shape, 1)
    gap = (gap + FRONT).astype(F32)
    for j in range(*block):
        window = pl.ds(j * plan.size, 128)
        scores = lax.dot_general(
            queries[plan.piece(j), :],
            kv[window, :both],
            (((1,), (1,)), ((), ())),
            preferred_element_type=F32,
        )
        weights = jnp.where(gap <= tcol[plan.piece(j), :], scores * fade[...], 0.0).astype(BF16)
        inner.append(jnp.dot(weights, kv[window, both:], preferred_element_type=F32))
    at = plan.span(block)
    low = plan.first_sequence(block[0] * plan.size) // 2
    high = plan.last_sequence(block[1] * plan.size - 1) // 2 + 1
    q, owner = queries[at, :], bcol[at, :]
    lane = lax.broadcasted_iota(jnp.int32, (q.shape[0], both), 1)
    pick = owner - jnp.where(lane < plan.key_dim, 0.0, 1.0).astype(BF16)
    zero = jnp.zeros_like(q)
    spread = [jnp.where(pick == jnp.asarray(2.0 * c, BF16), q, zero) for c in range(low, high)]
    middle = (low + high) // 2
    carried = None
    for first, last in ((low, middle), (middle, high)):
        term = jnp.dot(
            jnp.concatenate(spread[first - low : last - low], axis=1),
            halves[first * both : last * both, :],
            preferred_element_type=F32,
        )
        carried = term if carried is None else carried + term
    retained = jnp.concatenate(inner, axis=0) + carried * jnp.exp(rate * (tcol[at, :] + 1.0))
    inv = lax.rsqrt(jnp.mean(retained * retained, axis=-1, keepdims=True) + NORM_EPSILON)
    return (retained * inv * gate[at, :]).astype(BF16)


class Scatter:
    def __init__(self, ring, h_pair, w_pair, outbox, inbox, parts, sems):
        self.ring, self.plan = ring, ring.plan
        self.h_pair, self.w_pair, self.outbox, self.inbox, self.parts = h_pair, w_pair, outbox, inbox, parts
        self.out, self.recv, self.pair_recv = sems

    def offer(self, k):
        rows, depth = self.plan.span(self.plan.blocks[k]), self.plan.value_dim
        return remote(
            self.h_pair.at[rows, pl.ds(0, depth)],
            self.h_pair.at[rows, pl.ds(depth, depth)],
            self.out.at[1],
            self.pair_recv.at[k],
            self.ring.partner,
        )

    def hop(self, j, way, i):
        return remote(
            self.outbox.at[j, way, i - 1],
            self.inbox.at[j, way, i - 1],
            self.out.at[0],
            self.recv.at[j, way, i - 1],
            self.ring.next[way],
        )

    def prepare(self, k, distance):
        plan = self.plan
        ways = (0, 1) if 0 < distance < plan.far else (0,)
        at = plan.span(plan.blocks[k])
        columns = []
        for way in ways:
            target = self.ring.ahead(way, distance)
            columns.append(self.w_pair[:, pl.ds(pl.multiple_of(target * plan.width, plan.width), plan.width)])
        part = jnp.dot(
            self.h_pair[at, :], jnp.concatenate(columns, axis=1), preferred_element_type=F32
        )
        for way in ways:
            self.parts[way, distance % 2, at, :] = part[:, way * plan.width : (way + 1) * plan.width]

    def begin(self, k):
        plan = self.plan
        self.offer(k).wait_recv()
        self.prepare(k, plan.far)
        for j in range(*plan.blocks[k]):
            way = j % 2
            self.outbox[j, way, 0] = self.parts[0, plan.far % 2, plan.piece(j), :].astype(BF16)
            self.hop(j, way, 1).start()
        self.prepare(k, plan.far - 1)
        for j in range(*plan.blocks[k]):
            way = 1 - j % 2
            self.outbox[j, way, 0] = self.parts[way, (plan.far - 1) % 2, plan.piece(j), :].astype(BF16)
            self.hop(j, way, 1).start()
        self.prepare(k, plan.far - 2)

    def arrive(self, j, way, i):
        distance = self.plan.reach(j, way) - i
        if distance <= 0:
            return
        self.hop(j, way, i).wait_recv()
        part = self.parts[way, distance % 2, self.plan.piece(j), :] + self.inbox[j, way, i - 1].astype(F32)
        self.outbox[j, way, i] = part.astype(BF16)
        self.hop(j, way, i + 1).start()

    def round(self, k, i):
        plan = self.plan
        for j in range(*plan.blocks[k]):
            for way in (0, 1):
                self.arrive(j, way, i)
        if plan.far - 2 - i >= 0:
            self.prepare(k, plan.far - 2 - i)

    def last(self, j):
        plan = self.plan
        total = self.parts[0, 0, plan.piece(j), :]
        for way in (1 - j % 2, j % 2):
            reach = plan.reach(j, way)
            self.hop(j, way, reach).wait_recv()
            total = total + self.inbox[j, way, reach - 1].astype(F32)
        return total.astype(BF16).astype(F32)

    def drain(self, whole):
        every = whole.at[:, pl.ds(0, (self.plan.m - 1) * self.plan.width)]
        remote(every, every, self.out.at[0], self.pair_recv.at[0], self.ring.partner).wait_send()
        half = self.h_pair.at[:, pl.ds(0, self.plan.value_dim)]
        remote(half, half, self.out.at[1], self.pair_recv.at[0], self.ring.partner).wait_send()


def whole_kernel(plan, *refs):
    (lens_smem, powers, rates, lens_ref, tokens, rope, *rest) = refs
    gains, raw, outs_w, states_in, (mixed, *states), scratch = (
        (rest[0], rest[7]),
        (rest[1:5], rest[8:12]),
        (rest[5], rest[12]),
        (rest[6], rest[13]),
        rest[14:17],
        rest[17:],
    )
    (x, x1, y, whole, wcats, turned, w_pairs, total, squares, table, gate, tcol, bcol, queries) = scratch[:14]
    (kv, halves, hot, onward, tgt, parts, outbox, inbox, h_pair, trow, bounds, fade) = scratch[14:26]
    load, pair_w = scratch[26:28]
    sems = scratch[28:]
    ring = Ring(plan)
    ring.greet()
    depth, both = plan.value_dim, 2 * plan.key_dim
    rate = rates[0, ring.me]

    loads = {}
    for i in range(2):
        wq, wk, wv, wg = raw[i]
        targets = (
            (wq, turned.at[i, 0]),
            (wk, turned.at[i, 1]),
            (wv, wcats.at[i, :, pl.ds(both, depth)]),
            (wg, wcats.at[i, :, pl.ds(both + depth, depth)]),
            (outs_w[i], w_pairs.at[i, pl.ds(0, depth), :]),
            (states_in[i], states[i]),
        )
        for k, (source, target) in enumerate(targets):
            loads[i, k] = pltpu.make_async_copy(source, target, load.at[i, k])

    def swap(i):
        return remote(
            w_pairs.at[i, pl.ds(0, depth), :],
            w_pairs.at[i, pl.ds(depth, depth), :],
            pair_w.at[0, i],
            pair_w.at[1, i],
            ring.partner,
        )

    gathers = [Gather(ring, (x, x1)[i], whole, sems[:3]) for i in range(2)]
    scatters = [
        Scatter(ring, h_pair, w_pairs.at[i], outbox, inbox, parts, sems[3:])
        for i in range(2)
    ]
    projections = [Projection(gathers[i], gains[i], wcats.at[i], total, squares) for i in range(2)]

    for k in range(6):
        loads[0, k].start()
    met = []

    def send(j):
        if not met:
            ring.met()
            met.append(1)
        gathers[0].begin(j)

    pack_rows(plan, lens_ref, tokens, x, trow, bounds, send)
    for k in range(6):
        loads[1, k].start()
    loads[0, 0].wait()
    loads[0, 1].wait()

    loads[0, 2].wait()
    loads[0, 3].wait()
    shape = (plan.size, 128)
    gap = lax.broadcasted_iota(jnp.int32, shape, 0) - lax.broadcasted_iota(jnp.int32, shape, 1)
    gap = (gap + FRONT).astype(F32)
    near = (gap >= 0.0) & (gap < float(plan.block_len))
    fade[...] = jnp.where(near, 0.5 * jnp.exp(rate * jnp.maximum(gap, 0.0)), 0.0)
    kv[:FRONT, :] = jnp.zeros((FRONT, kv.shape[1]), BF16)
    kv[FRONT + plan.rows :, :] = jnp.zeros((plan.long - FRONT - plan.rows, kv.shape[1]), BF16)
    y[:FRONT, :] = jnp.zeros((FRONT, plan.width), BF16)
    y[FRONT + plan.rows :, :] = jnp.zeros((plan.long - FRONT - plan.rows, plan.width), BF16)
    loads[0, 5].wait()
    loads[0, 4].wait()
    swap(0).start()

    def step(i, ks, h, work):
        for k in ks:
            for j in range(*plan.blocks[k]):
                for way in (0, 1):
                    gathers[i].arrive(j, way, h)
            projections[i].add(k, h - 1)
            if work:
                act = work.pop(0)
                if act:
                    act()

    def retain(i, k):
        projections[i].finish(plan.blocks[k], table, queries, kv, gate)
        h_pair[plan.span(plan.blocks[k]), :depth] = retention_block(
            plan, rate, plan.blocks[k], queries, kv, gate, tcol, bcol, fade, halves
        )
        scatters[i].offer(k).start()

    def turn(i, ks, r, work):
        for k in ks:
            scatters[i].round(k, r)
            if r > (2 if k in leading else 1) and work:
                work.pop(0)()

    def flush(work):
        while work:
            act = work.pop(0)
            if act:
                act()

    leading, trailing, far = plan.leading, plan.trailing, plan.far

    def middle(i, h):
        swapped = False
        for n, k in enumerate(leading):
            retain(i, k)
            if n > 0:
                if not swapped:
                    swap(i).wait_recv()
                    swapped = True
                scatters[i].begin(leading[n - 1])
            if h <= far:
                step(i, trailing, h, [])
                h += 1
        while h <= far:
            step(i, trailing, h, [])
            h += 1
        early = list(leading)
        for n, k in enumerate(trailing):
            retain(i, k)
            scatters[i].begin(leading[-1] if n == 0 else trailing[n - 1])
            turn(i, early[:1], 1, [])
            early = early[1:]
        gathers[i].drain()
        turn(i, early, 1, [])
        scatters[i].begin(trailing[-1])

    def back(i, work, finish, between):
        for r in range(2, far):
            behind = list(trailing)
            for n, k in enumerate(leading):
                turn(i, [k], r, work)
                if n > 0 and behind:
                    turn(i, [behind.pop(0)], r - 1, work)
            turn(i, behind, r - 1, work)
        for k in leading:
            for j in range(*plan.blocks[k]):
                finish(j, scatters[i].last(j))
        turn(i, trailing, far - 1, work)
        flush(work)
        between()
        for k in trailing:
            for j in range(*plan.blocks[k]):
                finish(j, scatters[i].last(j))

    def every(first, last, unit_work):
        def act():
            @pl.loop(first, last)
            def _(u):
                unit_work(u)

        return act

    units = plan.units

    def update(i, times):
        body = lambda u: state_unit(plan, lens_smem, powers, ring.me, hot, kv, onward, states[i], u)
        return spread_out(units, times, body)

    def halve(i):
        return every(0, units, lambda u: split_unit(plan, states[i], halves, u))

    slot_body = lambda u: slot_unit(plan, rate, lens_ref, tgt, onward, hot, u)
    row_body = lambda u: row_unit(plan, bounds, rope, tcol, bcol, table, u)
    spread_out = lambda total, times, body: [
        every(total * k // times, total * (k + 1) // times, body) for k in range(times)
    ]
    rows_work = spread_out(plan.pieces, 2, row_body)
    first_work = [rows_work[0], None, rows_work[1], None, halve(0)]

    def after_first(j, mix):
        at = plan.piece(j)
        x1[at, :] = (x[at, :].astype(F32) + mix).astype(BF16)
        gathers[1].begin(j)

    def ready_second():
        for k in range(6):
            loads[1, k].wait()
        swap(1).start()

        @pl.loop(0, wcats.shape[1] // 128)
        def _(u):
            fill_unit(turned.at[1, 0], turned.at[1, 1], wcats.at[1], u)

    fills = spread_out(
        wcats.shape[1] // 128,
        len(leading),
        lambda u: fill_unit(turned.at[0, 0], turned.at[0, 1], wcats.at[0], u),
    )
    for n, k in enumerate(leading):
        if n > 0:
            for j in range(*plan.blocks[k]):
                for way in (0, 1):
                    gathers[0].arrive(j, way, 1)
        fills[n]()
        if n == 0:
            for j in range(*plan.blocks[k]):
                for way in (0, 1):
                    gathers[0].arrive(j, way, 1)
    for k in trailing:
        for j in range(*plan.blocks[k]):
            gathers[0].begin(j)
    for k in leading:
        projections[0].add(k, 0)
    for h in range(2, far):
        step(0, leading, h, first_work)
    step(0, trailing, 1, first_work)
    step(0, leading, far, first_work)
    flush(first_work)
    middle(0, 2)

    second_work = []
    for act in [halve(1)] + update(0, 6):
        second_work += [act, None]
    back(
        0,
        [ready_second] + spread_out(units, 4, slot_body),
        after_first,
        lambda: step(1, leading, 1, []),
    )
    scatters[0].drain(whole)
    swap(0).wait_send()
    for h in range(2, far):
        step(1, leading, h, second_work)
        step(1, trailing, h - 1, second_work)
    step(1, leading, far, second_work)
    flush(second_work)

    def after_second(j, mix):
        at = plan.piece(j)
        y[pl.ds(FRONT + j * plan.size, plan.size), :] = (x1[at, :].astype(F32) + mix).astype(BF16)

    middle(1, far - 1)
    back(1, update(1, 6), after_second, lambda: None)
    scatters[1].drain(whole)
    swap(1).wait_send()
    many = next(k for k in (3, 2, 1) if plan.units % k == 0)

    @pl.loop(0, plan.units // many)
    def _(u):
        at = pl.ds(pl.multiple_of(u * many * plan.unit, plan.unit), many * plan.unit)
        spread = jnp.dot(hot[at, :], y[...], preferred_element_type=F32)
        live = jnp.concatenate([tgt[at, :]] * (plan.width // 128), axis=1) >= 0.0
        mixed[at, :] = jnp.where(live, spread, tokens[at, :].astype(F32)).astype(BF16)


def fused(plan, heads, lengths, tokens, first, second):
    total_heads = heads
    logs = np.log(1.0 - 2.0 ** (-1.5 - 6.0 * np.arange(total_heads) / (total_heads - 1)))
    powers = np.exp(logs[:, None] * np.arange(plan.block_len + 1)[None, :]).astype(np.float32)
    half = plan.key_dim // 2
    inverse = np.float32(ROPE_BASE) ** (-np.arange(half, dtype=np.float32) / np.float32(half))
    positions = PAST_LEN + np.arange(plan.block_len, dtype=np.float32)
    angles = (positions[:, None] * inverse.astype(np.float32)[None, :]).astype(np.float64)
    cosines, sines = np.cos(angles), np.sin(angles)
    cosines = np.concatenate([cosines, cosines], axis=1)
    sines = np.concatenate([-sines, sines], axis=1)
    scale = plan.key_dim**-0.5
    rope = np.concatenate([cosines, cosines * scale, sines, sines * scale], axis=1).astype(np.float32)
    stacked, rest = [], rope
    for _ in range(3):
        stacked.append(rest.astype(jnp.bfloat16))
        rest = rest - stacked[-1].astype(np.float32)
    rope = np.zeros((128, rope.shape[1]), jnp.bfloat16)
    rope[: 3 * plan.block_len] = np.concatenate(stacked, axis=0)

    n, rows, width = plan.n, plan.rows, plan.width
    wide, both = 2 * plan.key_dim + 2 * plan.value_dim, 2 * plan.key_dim
    depth = plan.value_dim
    model = n * width
    state_shape = (plan.batch, plan.key_dim, plan.value_dim)
    vmem = lambda shape, kind: pltpu.VMEM(shape, kind)
    dma = lambda *shape: pltpu.SemaphoreType.DMA(shape)
    scratch = [
        vmem((rows, width), BF16),
        vmem((rows, width), BF16),
        vmem((plan.long, width), BF16),
        vmem((rows, model), BF16),
        vmem((2, model, wide), BF16),
        vmem((2, 2, plan.key_dim, model), BF16),
        vmem((2, 2 * depth, model), BF16),
        vmem((rows, wide), F32),
        vmem((rows, 128), F32),
        vmem((rows, 2 * both), F32),
        vmem((rows, depth), F32),
        vmem((rows, 128), F32),
        vmem((rows, 128), BF16),
        vmem((rows, both), BF16),
        vmem((plan.long, both + depth), BF16),
        vmem((plan.batch * plan.key_dim, depth), BF16),
        vmem((plan.slots, plan.long), BF16),
        vmem((plan.slots, 128), F32),
        vmem((plan.slots, 128), F32),
        vmem((2, 2, rows, width), F32),
        vmem((plan.pieces, 2, plan.far, plan.size, width), BF16),
        vmem((plan.pieces, 2, plan.far, plan.size, width), BF16),
        vmem((rows, 2 * depth), BF16),
        vmem((8, plan.slots), F32),
        vmem((16, plan.batch), F32),
        vmem((plan.size, 128), F32),
        dma(2, 6),
        dma(2, 2),
    ]
    scratch += [dma(2), dma(plan.pieces, 2, plan.far), dma(len(plan.blocks), plan.far + 1)]
    scratch += [dma(2), dma(plan.pieces, 2, plan.far), dma(len(plan.blocks))]
    spec = lambda space: pl.BlockSpec(memory_space=space)
    inside, outside, scalars = spec(pltpu.VMEM), spec(pltpu.HBM), spec(pltpu.SMEM)

    def group(gain, query, key, value, gate, out, state):
        far = [
            pltpu.with_memory_space_constraint(a, pltpu.HBM)
            for a in (query.T, key.T, value, gate, out, state.reshape(state_shape))
        ]
        return (gain[None], *far)

    block_specs = [inside] + [outside] * 6

    mixed, one, two = pl.pallas_call(
        functools.partial(whole_kernel, plan),
        out_shape=[
            pltpu.VMEM((plan.slots, width), BF16),
            pltpu.VMEM(state_shape, F32),
            pltpu.VMEM(state_shape, F32),
        ],
        in_specs=[scalars] * 3 + [inside] * 3 + block_specs * 2,
        out_specs=[inside, inside, inside],
        scratch_shapes=scratch,
        compiler_params=pltpu.CompilerParams(
            collective_id=0, has_side_effects=True, vmem_limit_bytes=48 * 2**20
        ),
    )(
        lengths,
        jnp.asarray(powers),
        jnp.asarray(logs.astype(np.float32)[None, :]),
        lengths[None, :],
        tokens,
        jnp.asarray(rope),
        *group(*first),
        *group(*second),
    )
    return mixed, one.reshape(first[-1].shape), two.reshape(second[-1].shape)


def unpacked(lengths, tokens, first, second):
    batch_size, head_count, key_dim, value_dim = first[-1].shape
    slots = tokens.shape[0]
    block_len = slots // batch_size
    table = jnp.tile(rope_tables(block_len, key_dim), (batch_size, 1))
    x, states = tokens, []
    for gain, query, key, value, gate, out, state in (first, second):
        qk = []
        for weight in (query, key):
            qk.append(weight.reshape(weight.shape[0], head_count, key_dim))
        x, new_state = plain_block(x, lengths, gain, qk, value, gate, out, state, table)
        states.append(new_state)
    return (x, *states)


def shards(
    tokens,
    lengths,
    gain_first,
    query_first,
    key_first,
    value_first,
    gate_first,
    out_first,
    state_first,
    gain_second,
    query_second,
    key_second,
    value_second,
    gate_second,
    out_second,
    state_second,
):
    n = lax.axis_size("tp")
    batch_size, head_count, key_dim, value_dim = state_first.shape
    slots, width = tokens.shape
    block_len = slots // batch_size
    rows = LIVE_TOTAL
    lengths = lengths.astype(jnp.int32)
    first = (gain_first, query_first, key_first, value_first, gate_first, out_first, state_first)
    second = (gain_second, query_second, key_second, value_second, gate_second, out_second, state_second)
    pieces = next((p for p in (10, 8, 6, 4) if rows % (16 * p) == 0 and rows // p <= 128 - FRONT), 0)
    fits = (
        n >= 12
        and n % 4 == 0
        and pieces >= 8
        and head_count == 1
        and width == 128
        and value_dim == 128
        and key_dim == 64
        and block_len <= FRONT
        and 128 % (2 * block_len) == 0
        and 3 * block_len <= 128
        and batch_size <= 128
        and batch_size % 2 == 0
        and slots % 128 == 0
    )
    if not fits:
        return unpacked(lengths, tokens, first, second)
    plan = Plan(n, rows, pieces, batch_size, block_len, key_dim, value_dim, width)
    return fused(plan, n * head_count, lengths, tokens, first, second)


def solution(mesh):
    heads = P(None, "tp")
    state = P("grp", "tp", None, None)
    block = (P(), heads, heads, heads, heads, P("tp", None), state)
    in_specs = (P("grp", "tp"), P("grp")) + block + block
    out_specs = (P("grp", "tp"), state, state)
    return jax.shard_map(shards, mesh=mesh, in_specs=in_specs, out_specs=out_specs, check_vma=False)
```
